512 devices in a mesh: sp: 64 (over z, y), tp: 4 (over x), dp: 2 (over core).
Axes of the slice: x: 4, y: 8, z: 8, core: 2. Of those that a mesh axis runs over, the one named last changes fastest.
Arguments:
- latent: bfloat16 [2, 16384, 2048], P('dp', 'sp'), may hold values from -1.5 to 1.5
- condition: bfloat16 [2, 2048], P('dp', 'sp'), may hold values from -6 to 6
- context: bfloat16 [2, 1024, 2048], P('dp', 'sp'), may hold values from -6 to 6
- context_code: bfloat16 [2048], P('sp'), may hold values from -6 to 6
- shift_weight: bfloat16 [2048, 2048], P('sp', 'tp'), may hold values from -0.125 to 0.125
- scale_weight: bfloat16 [2048, 2048], P('sp', 'tp'), may hold values from -0.125 to 0.125
- gate_weight: bfloat16 [2048, 2048], P('sp', 'tp'), may hold values from -0.125 to 0.125
- norm_gain: float32 [2048], replicated, may hold values from 0.1 to 1.9
- query_weight: bfloat16 [2048, 1024], P(None, 'tp'), may hold values from -0.125 to 0.125
- key_weight: bfloat16 [2048, 256], P(None, 'tp'), may hold values from -0.125 to 0.125
- value_weight: bfloat16 [2048, 256], P(None, 'tp'), may hold values from -0.125 to 0.125
- output_weight: bfloat16 [1024, 2048], P('tp'), may hold values from -0.75 to 0.75
- query_gain: float32 [64], replicated, may hold values from 1 to 5.5
- key_gain: float32 [64], replicated, may hold values from 1 to 5.5
- context_bias: float32 [16], P('tp'), may hold values from 0.5 to 2
Outputs:
- updated: bfloat16 [2, 16384, 2048], P('dp', 'sp')
The draws below stay inside these ranges and needn't reach their ends.
All inputs are finite; a program needn't handle non-finite values.
Results may differ from the reference program's by a relative error of at most 0.01405.
The reference program's roundings to bfloat16 on the way count: a program that leaves them out, or rounds other values in their place, can miss the bound.
Values may be sent and summed in bfloat16 or wider, within the bound.
A program may use at most 64 MiB of HBM per device.

```python
import math
import jax
import jax.numpy as jnp
from jax import lax

D = 2048
HEADS = 16
KV_HEADS = 4
HEAD = 64
GRID_W = 64
CTX = 1024
SAMPLES = 2
SEQ = 16384


def gain_draw(key, salt):
    fresh = jax.random.fold_in(key, salt)
    return jnp.exp(jax.random.uniform(fresh, (HEAD,), jnp.float32, 0.0, math.log(2.2)))


def draw_query_gain(key, part):
    return gain_draw(key, 17)


def draw_key_gain(key, part):
    return gain_draw(key, 29)


def shard_levels(rng, dims, cuts, smallest, largest):
    gain, own = 1.0, jax.random.fold_in(rng, 6)
    for dim, blocks in cuts:
        draws = jnp.exp(jax.random.uniform(jax.random.fold_in(own, dim), (blocks,), jnp.float32, smallest / len(cuts), largest / len(cuts)))
        gain = gain * jnp.repeat(draws, dims[dim] // blocks).reshape([-1 if axis == dim else 1 for axis in range(len(dims))])
    return gain


def centred(stream_key, dims, spread, bound, split=(), kind=jnp.bfloat16):
    entries = spread * jax.random.normal(stream_key, dims, jnp.float32)
    if split:
        entries = entries * shard_levels(stream_key, dims, split, -0.22, 0.18)
    return jnp.clip(entries, -bound, bound).astype(kind)


def setup_inputs(seed: int = 0) -> dict:
    key_of = jax.random.split(jax.random.key(seed), 16)
    latent = centred(key_of[0], (SAMPLES, SEQ, D), 0.25, 1.5, ((0, 2), (1, 64)))
    condition = centred(key_of[1], (SAMPLES, D), 1.0, 6.0, ((0, 2), (1, 64)))
    context = centred(key_of[2], (SAMPLES, CTX, D), 1.0, 6.0, ((0, 2), (1, 64)))
    context_code = centred(key_of[3], (D,), 1.0, 6.0, ((0, 64),))
    shift_weight = centred(key_of[4], (D, D), D ** -0.5, 0.125, ((0, 64), (1, 4)))
    scale_weight = centred(key_of[5], (D, D), D ** -0.5, 0.125, ((0, 64), (1, 4)))
    gate_weight = centred(key_of[6], (D, D), D ** -0.5, 0.125, ((0, 64), (1, 4)))
    norm_gain = jnp.clip(1.0 + 0.18 * jax.random.normal(key_of[7], (D,), jnp.float32), 0.1, 1.9)
    query_weight = centred(key_of[8], (D, HEADS * HEAD), D ** -0.5, 0.125, ((1, 4),))
    key_weight = centred(key_of[9], (D, KV_HEADS * HEAD), D ** -0.5, 0.125, ((1, 4),))
    value_weight = centred(key_of[10], (D, KV_HEADS * HEAD), D ** -0.5, 0.125, ((1, 4),))
    output_weight = centred(key_of[11], (HEADS * HEAD, D), (HEADS * HEAD // 16) ** -0.5, 0.75, ((0, 4),))
    query_gain = draw_query_gain(jax.random.fold_in(key_of[15], 71), 0)
    key_gain = draw_key_gain(jax.random.fold_in(key_of[15], 71), 0)
    context_bias = jnp.clip(0.5 + 1.5 * jax.random.uniform(key_of[14], (HEADS,), jnp.float32) ** shard_levels(key_of[14], (HEADS,), ((0, 4),), -0.2, 0.2), 0.5, 2.0)
    return {"latent": latent, "condition": condition, "context": context, "context_code": context_code, "shift_weight": shift_weight, "scale_weight": scale_weight, "gate_weight": gate_weight, "norm_gain": norm_gain, "query_weight": query_weight, "key_weight": key_weight, "value_weight": value_weight, "output_weight": output_weight, "query_gain": query_gain, "key_gain": key_gain, "context_bias": context_bias}


norm_eps = 1e-06
rope_base = 10000.0

def rotary_tables(position):
    grid_row = (position // GRID_W).astype(jnp.float32)
    grid_col = (position % GRID_W).astype(jnp.float32)
    quarter = HEAD // 4
    inverse = rope_base ** (-jnp.arange(quarter, dtype=jnp.float32) / quarter)
    angles = jnp.concatenate([grid_row[:, None] * inverse, grid_col[:, None] * inverse], axis=-1)
    return (jnp.cos(angles), jnp.sin(angles))

def head_norm(values, gain_row):
    return values * lax.rsqrt(lax.optimization_barrier(jnp.mean(values * values, axis=-1, keepdims=True)) + norm_eps) * gain_row

def rotate(values, cosine, sine_part):
    half_dim = values.shape[-1] // 2
    first_half = values[..., :half_dim]
    second_half = values[..., half_dim:]
    cos_rows = cosine[:, None, :]
    sin_rows = sine_part[:, None, :]
    return jnp.concatenate([first_half * cos_rows - second_half * sin_rows, second_half * cos_rows + first_half * sin_rows], axis=-1)

def modulated(tokens, gain_row, shift_row, scale_row):
    floats = tokens.astype(jnp.float32)
    normal = floats * lax.rsqrt(lax.optimization_barrier(jnp.mean(floats * floats, axis=-1, keepdims=True)) + norm_eps)
    return (normal * gain_row * (1.0 + scale_row) + shift_row).astype(jnp.bfloat16)

def attend(query_block, latent_keys, latent_values, context_keys, context_values, bias_value):
    score_scale = HEAD ** (-0.5)
    latent_scores = jnp.dot(query_block, latent_keys.T, preferred_element_type=jnp.float32) * score_scale
    context_scores = jnp.dot(query_block, context_keys.T, preferred_element_type=jnp.float32) * score_scale + bias_value
    row_max = jnp.maximum(latent_scores.max(axis=1), context_scores.max(axis=1))[:, None]
    latent_exp = jnp.exp(latent_scores - row_max)
    context_exp = jnp.exp(context_scores - row_max)
    totals = latent_exp.sum(axis=1) + context_exp.sum(axis=1)
    summed = jnp.dot(latent_exp.astype(jnp.bfloat16), latent_values, preferred_element_type=jnp.float32)
    summed = summed + jnp.dot(context_exp.astype(jnp.bfloat16), context_values, preferred_element_type=jnp.float32)
    return (summed / totals[:, None]).astype(jnp.bfloat16)

def reference(latent, condition, context, context_code, shift_weight, scale_weight, gate_weight, norm_gain, query_weight, key_weight, value_weight, output_weight, query_gain, key_gain, context_bias):
    cosine, sine_part = rotary_tables(jnp.arange(SEQ, dtype=jnp.int32))
    group_size = HEADS // KV_HEADS
    query_block = math.gcd(SEQ, 512)
    context_act = jax.nn.silu(context_code.astype(jnp.float32)).astype(jnp.bfloat16)
    context_shift = jnp.dot(context_act, shift_weight, preferred_element_type=jnp.float32)
    context_scale = jnp.dot(context_act, scale_weight, preferred_element_type=jnp.float32)
    results = []
    for sample in range(SAMPLES):
        activated = jax.nn.silu(condition[sample].astype(jnp.float32)).astype(jnp.bfloat16)
        latent_shift = jnp.dot(activated, shift_weight, preferred_element_type=jnp.float32)
        latent_scale = jnp.dot(activated, scale_weight, preferred_element_type=jnp.float32)
        latent_gate = jnp.dot(activated, gate_weight, preferred_element_type=jnp.float32)
        normed = modulated(latent[sample], norm_gain, latent_shift, latent_scale)
        queries = jnp.dot(normed, query_weight, preferred_element_type=jnp.float32).reshape(SEQ, HEADS, HEAD)
        queries = rotate(head_norm(queries, query_gain), cosine, sine_part).astype(jnp.bfloat16)
        latent_keys = jnp.dot(normed, key_weight, preferred_element_type=jnp.float32).reshape(SEQ, KV_HEADS, HEAD)
        latent_keys = rotate(head_norm(latent_keys, key_gain), cosine, sine_part).astype(jnp.bfloat16)
        latent_values = jnp.dot(normed, value_weight, preferred_element_type=jnp.float32)
        latent_values = latent_values.reshape(SEQ, KV_HEADS, HEAD).astype(jnp.bfloat16)
        context_normed = modulated(context[sample], norm_gain, context_shift, context_scale)
        context_keys = jnp.dot(context_normed, key_weight, preferred_element_type=jnp.float32).reshape(CTX, KV_HEADS, HEAD)
        context_keys = head_norm(context_keys, key_gain).astype(jnp.bfloat16)
        context_values = jnp.dot(context_normed, value_weight, preferred_element_type=jnp.float32)
        context_values = context_values.reshape(CTX, KV_HEADS, HEAD).astype(jnp.bfloat16)
        mixed = jnp.zeros((SEQ, D), jnp.float32)
        for kv_head in range(KV_HEADS):
            outputs = []
            for head_index in range(kv_head * group_size, (kv_head + 1) * group_size):
                head_out = lax.map(partial_attend(latent_keys[:, kv_head], latent_values[:, kv_head], context_keys[:, kv_head], context_values[:, kv_head], context_bias[head_index]), queries[:, head_index].reshape(SEQ // query_block, query_block, HEAD))
                outputs.append(head_out.reshape(SEQ, HEAD))
            attended = jnp.concatenate(outputs, axis=1)
            rows_start = kv_head * group_size * HEAD
            weight_rows = output_weight[rows_start:rows_start + group_size * HEAD]
            partial_sum = jnp.dot(attended, weight_rows, preferred_element_type=jnp.float32).astype(jnp.bfloat16)
            mixed = mixed + partial_sum.astype(jnp.float32)
        updated = latent[sample].astype(jnp.float32) + latent_gate * mixed
        results.append(updated.astype(jnp.bfloat16))
    return jnp.stack(results)

def partial_attend(latent_keys, latent_values, context_keys, context_values, bias_value):

    def attend_block(query_block):
        return attend(query_block, latent_keys, latent_values, context_keys, context_values, bias_value)
    return attend_block
```

```python
import functools
import math

import jax
import jax.numpy as jnp
from jax import lax
from jax.experimental import pallas as pl
from jax.experimental.pallas import tpu as pltpu
from jax.sharding import PartitionSpec as P

MESH = pl.DeviceIdType.MESH
F32 = jnp.float32
BF16 = jnp.bfloat16
EPS = 1e-6
ROPE_BASE = 10000.0
GRID_W = 64
RING = 8
XN = 4
TOK = 256
CTXT = 16
D = 2048
HD = 64
NH = 4
QC = NH * HD
LOG2E = 1.4426950408889634


def dot(a, b):
    return jnp.dot(a, b, preferred_element_type=F32)


def kernel(
    latent_h, cond_h, context_h, code_h, shw_h, scw_h, gaw_h, ngain_h, wq_h, wk_h, wv_h, wo_h, qg_h, kg_h, bias_h,
    out_h,
    lat, cond, ctx, code, shw, scw, gaw, ngain, wq, wk, wv, wo, qg, kg, bias,
    outv, normed, wkv, qbd, qctx, bufa, bufb, mst, lst, acc, att,
    ma, ma_y, ma_s, ma_z, ma_x, mb, mb_z, mb_s, mb_y, mb_x,
    lsem, osem, sa, ra, sb, rb, smod, rmod, swo, rwo, satt, ratt,
):
    sp = lax.axis_index("sp")
    x = lax.axis_index("tp")
    d = lax.axis_index("dp")
    z = sp // RING
    y = sp % RING
    sgn = 1 - 2 * d

    def at_y(k):
        return {"sp": z * RING + lax.rem(y + k + 2 * RING, RING)}

    def at_z(k):
        return {"sp": lax.rem(z + k + 2 * RING, RING) * RING + y}

    def at_x(k):
        return {"tp": lax.rem(x + k + 2 * XN, XN)}

    partner = {"dp": 1 - d}

    def remote(src, dst, ss, rs, dev):
        return pltpu.make_async_remote_copy(
            src_ref=src, dst_ref=dst, send_sem=ss, recv_sem=rs, device_id=dev, device_id_type=MESH
        )

    pairs = [
        (cond_h, cond), (code_h, code), (shw_h, shw), (scw_h, scw), (gaw_h, gaw),
        (latent_h, lat), (context_h, ctx), (ngain_h, ngain), (wk_h, wk), (wv_h, wv), (wq_h, wq),
        (qg_h, qg), (kg_h, kg), (bias_h, bias),
        (wo_h.at[:, 0 : D // 2], wo.at[x, 0]), (wo_h.at[:, D // 2 : D], wo.at[x, 1]),
    ]
    loads = [pltpu.make_async_copy(s, t, lsem.at[i]) for i, (s, t) in enumerate(pairs)]
    for c in loads:
        c.start()

    barrier = pltpu.get_barrier_semaphore()
    for k in range(1, RING):
        pl.semaphore_signal(barrier, inc=1, device_id=at_y(k), device_id_type=MESH)
        pl.semaphore_signal(barrier, inc=1, device_id=at_z(k), device_id_type=MESH)
    for k in range(1, XN):
        pl.semaphore_signal(barrier, inc=1, device_id=at_x(k), device_id_type=MESH)
    pl.semaphore_signal(barrier, inc=1, device_id=partner, device_id_type=MESH)

    for i in range(5):
        loads[i].wait()
    both = jnp.concatenate([cond[...], code[...]], axis=0).astype(F32)
    act = (both * (1.0 / (1.0 + jnp.exp(-both)))).astype(BF16)
    pshift = dot(act, shw[...])
    pscale = dot(act, scw[...])
    pgate = dot(act, gaw[...])
    for c in range(4):
        cols = slice(c * 128, (c + 1) * 128)
        ma[c : c + 1, :] = pshift[0:1, cols]
        ma[4 + c : 5 + c, :] = pscale[0:1, cols]
        ma[8 + c : 9 + c, :] = pgate[0:1, cols]
        mb[c : c + 1, :] = pshift[1:2, cols]
        mb[4 + c : 5 + c, :] = pscale[1:2, cols]
    ma[12:16, :] = jnp.zeros((4, 128), F32)

    pl.semaphore_wait(barrier, 2 * (RING - 1) + (XN - 1) + 1)

    def xa(src, dst, base, dev, k):
        return remote(src, dst.at[k], smod.at[base + k], rmod.at[base + k], dev)

    p1 = []
    for k in range(1, RING):
        p1.append(xa(ma, ma_y, 0, at_y(k), k))
        p1.append(xa(mb, mb_z, 8, at_z(k), k))
    for c in p1:
        c.start()

    for i in (14, 15):
        loads[i].wait()
    wo1 = [
        remote(wo.at[x, d], wo.at[x, d], swo.at[0], rwo.at[0], at_x(1)),
        remote(wo.at[x, d], wo.at[x, d], swo.at[1], rwo.at[1], at_x(-1)),
    ]
    for c in wo1:
        c.start()

    for i in (5, 6, 7, 8, 9):
        loads[i].wait()
    lf = lat[...].astype(F32)
    rms = lax.rsqrt(jnp.mean(lf * lf, axis=-1, keepdims=True) + EPS)
    cf = ctx[...].astype(F32)
    crms = lax.rsqrt(jnp.mean(cf * cf, axis=-1, keepdims=True) + EPS)
    wkv[...] = jnp.concatenate([wk[...], wv[...]], axis=1)
    qbd[...] = jnp.zeros(qbd.shape, BF16)
    qctx[...] = jnp.zeros(qctx.shape, BF16)
    mst[...] = jnp.full(mst.shape, -1e30, F32)
    lst[...] = jnp.zeros(lst.shape, F32)
    acc[...] = jnp.zeros(acc.shape, F32)
    fi = lax.broadcasted_iota(jnp.int32, (32, TOK), 0)
    ti = lax.broadcasted_iota(jnp.int32, (32, TOK), 1)
    grow = sp * (TOK // GRID_W) + ti // GRID_W
    gcol = ti % GRID_W
    gpos = jnp.where(fi < 16, grow, gcol).astype(F32)
    inv = jnp.exp((fi % 16).astype(F32) * (-math.log(ROPE_BASE) / 16.0))
    angle = gpos * inv
    cosv = jnp.cos(angle)
    sinv = jnp.sin(angle)

    for c in p1:
        c.wait()
    ta = ma[...]
    tb = mb[...]
    for k in range(1, RING):
        ta = ta + ma_y[k]
        tb = tb + mb_z[k]
    ma_s[0] = ta
    mb_s[0] = tb
    p2 = []
    for k in range(1, RING):
        p2.append(xa(ma_s.at[0], ma_z, 16, at_z(k), k))
        p2.append(xa(mb_s.at[0], mb_y, 24, at_y(k), k))
    for c in p2:
        c.start()
    for c in p2:
        c.wait()
    for k in range(1, RING):
        ta = ta + ma_z[k]
        tb = tb + mb_y[k]
    ma_x[x] = ta
    mb_x[x] = tb
    p3 = []
    for k in range(1, XN):
        p3.append(remote(ma_x.at[x], ma_x.at[x], smod.at[32 + k], rmod.at[32 + k], at_x(k)))
        p3.append(remote(mb_x.at[x], mb_x.at[x], smod.at[36 + k], rmod.at[36 + k], at_x(k)))
    for c in p3:
        c.start()
    for c in p3:
        c.wait()

    def vec(ref, row):
        return jnp.concatenate([ref[i, row + c : row + c + 1, :] for i in range(XN) for c in range(4)], axis=1)

    gain = ngain[...]
    lshift = vec(ma_x, 0)
    lscale = gain * (1.0 + vec(ma_x, 4))
    cshift = vec(mb_x, 0)
    cscale = gain * (1.0 + vec(mb_x, 4))
    normed[0:TOK, :] = (lat[...].astype(F32) * rms * lscale + lshift).astype(BF16)
    normed[TOK : TOK + CTXT, :] = (cf * crms * cscale + cshift).astype(BF16)

    kv = dot(normed[...], wkv[...])
    kvt = kv[0:TOK, :].T
    for i in (10, 11, 12, 13):
        loads[i].wait()
    eye = lax.broadcasted_iota(jnp.int32, (HD, HD), 0) == lax.broadcasted_iota(jnp.int32, (HD, HD), 1)
    qgain = jnp.sum(jnp.where(eye, qg[...], 0.0), axis=1, keepdims=True)
    kgain = jnp.sum(jnp.where(eye, kg[...], 0.0), axis=1, keepdims=True)

    def norm_rope(t, g):
        t = t * lax.rsqrt(jnp.mean(t * t, axis=0, keepdims=True) + EPS) * g
        a, b = t[0:32, :], t[32:64, :]
        return jnp.concatenate([a * cosv - b * sinv, b * cosv + a * sinv], axis=0)

    kt = norm_rope(kvt[0:HD, :], kgain)
    k2 = jnp.concatenate([kt, kt], axis=0).T
    low = lax.broadcasted_iota(jnp.int32, (HD, 128), 1) < HD
    vt = kvt[HD : 2 * HD, :].astype(BF16)
    bufa[0, 0:64, :] = jnp.where(low, k2[0:64], k2[64:128]).astype(BF16)
    bufb[0, 0:64, :] = jnp.where(low, k2[128:192], k2[192:256]).astype(BF16)
    bufa[0, 64:128, :] = vt[:, 0:128]
    bufb[0, 64:128, :] = vt[:, 128:256]
    ckv = kv[TOK : TOK + CTXT, :]
    lowc = lax.broadcasted_iota(jnp.int32, (CTXT, 128), 1) < HD
    csq = jnp.sum(jnp.where(lowc, ckv * ckv, 0.0), axis=1, keepdims=True) * (1.0 / HD)
    kg2 = jnp.concatenate([kg[...], kg[...]], axis=1)
    bufa[0, 128:144, :] = jnp.where(lowc, ckv * lax.rsqrt(csq + EPS) * kg2, ckv).astype(BF16)

    def send(src, dst, dev_a, dev_b):
        remote(bufa.at[src], bufa.at[dst], sa.at[dst], ra.at[dst], dev_a).start()
        remote(bufb.at[src], bufb.at[dst], sb.at[dst], rb.at[dst], dev_b).start()

    def arrived(s):
        remote(bufa.at[s], bufa.at[s], sa.at[s], ra.at[s], at_z(1)).wait_recv()
        remote(bufb.at[s], bufb.at[s], sb.at[s], rb.at[s], at_y(1)).wait_recv()

    def first(dst_, src_, s):
        send(src_, dst_, at_y(s), at_z(s))

    def second(src_, dst_, s):
        send(src_, dst_, at_z(s), at_y(s))

    def start_rows(i):
        nxt = {0: (1, 2), 1: (3,), 2: (4,), 3: (5,), 4: (6,), 5: (7,)}.get(i, ())
        for t in nxt:
            first(t, i, sgn if t % 2 == 1 else -sgn)
        base = (2 + i // 2) * 4 + i % 2
        second(i, base, sgn)
        second(i, base + 2, -sgn)

    start_rows(0)

    q = dot(normed[0:TOK, :], wq[...])
    qt = q.T
    for h in range(NH):
        qh = norm_rope(qt[h * HD : (h + 1) * HD, :], qgain).astype(BF16)
        qs = qh.astype(F32) * (LOG2E * HD**-0.5)
        hi = qs.astype(BF16)
        lo = (qs - hi.astype(F32)).astype(BF16)
        for t in range(2):
            cols = slice(t * 128, (t + 1) * 128)
            for r, part in ((0, hi), (128, lo)):
                qbd[2 * h + t, r : r + 64, 0:128] = part[:, cols]
                qbd[2 * h + t, r + 64 : r + 128, 128:256] = part[:, cols]
        qctx[h, 0:64, :] = hi
        qctx[h, 128:192, :] = lo

    def absorb(h, mnew, rowsum, prod):
        alpha = jnp.exp2(mst[h] - mnew)
        mst[h] = mnew
        lst[h] = lst[h] * alpha[0:1, :] + rowsum
        acc[h] = acc[h] * alpha[0:1, :] + prod

    def step(it, carry):
        base = it * 4

        @pl.when(it == 0)
        def _():
            for i in (1, 2, 3):
                arrived(i)
                start_rows(i)

        @pl.when(it == 1)
        def _():
            for i in (4, 5, 6, 7):
                arrived(i)
                start_rows(i)

        @pl.when((it >= 2) & (it < 10))
        def _():
            for k in range(4):
                arrived(base + k)
                second(base + k, base + k + 16, sgn if k < 2 else -sgn)

        @pl.when((it >= 10) & (it < 14))
        def _():
            for k in range(4):
                arrived(base + k)
                if k < 2:
                    second(base + k, 56 + 2 * (it - 10) + k, sgn)

        @pl.when(it >= 14)
        def _():
            for k in range(4):
                arrived(base + k)

        @pl.when(it == 8)
        def _():
            for c in wo1:
                c.wait()
            left = lax.rem(x + XN - 1, XN)
            right = lax.rem(x + 1, XN)
            remote(wo.at[left, d, 0:128], wo.at[left, d, 0:128], swo.at[2], rwo.at[2], at_x(1)).start()
            remote(wo.at[right, d, 128:256], wo.at[right, d, 128:256], swo.at[3], rwo.at[3], at_x(-1)).start()
            remote(wo.at[left, d], wo.at[left, d], swo.at[4], rwo.at[4], partner).start()
            remote(wo.at[right, d], wo.at[right, d], swo.at[5], rwo.at[5], partner).start()

        @pl.when(it == 14)
        def _():
            far = lax.rem(x + 2, XN)
            remote(wo.at[far, d, 0:128], wo.at[far, d, 0:128], swo.at[2], rwo.at[2], at_x(1)).wait()
            remote(wo.at[far, d, 128:256], wo.at[far, d, 128:256], swo.at[3], rwo.at[3], at_x(-1)).wait()
            remote(wo.at[far, d], wo.at[far, d], swo.at[6], rwo.at[6], partner).start()

        keys = jnp.concatenate(
            [bufa[pl.ds(base, 4), 0:64, :].reshape(256, 128), bufb[pl.ds(base, 4), 0:64, :].reshape(256, 128)], axis=0
        )
        keys = jnp.concatenate([keys, keys], axis=1)
        vals = jnp.concatenate(
            [bufa[base + k, 64:128, :] for k in range(4)] + [bufb[base + k, 64:128, :] for k in range(4)], axis=1
        )
        for h in range(NH):
            ps = []
            ms = []
            sums = []
            mold = mst[h]
            for t in range(2):
                s = dot(keys, qbd[2 * h + t])
                m = jnp.max(s.reshape(64, 8, 256), axis=0)
                m = jnp.maximum(m[:, 0:128], m[:, 128:256])
                m = jnp.max(m, axis=0, keepdims=True)
                m = jnp.maximum(m, mold[0:1, t * 128 : (t + 1) * 128])
                e = jnp.exp2(s - jnp.concatenate([m, m], axis=1))
                r = jnp.sum(e.reshape(64, 8, 256), axis=0)
                sums.append(r[:, 0:128] + r[:, 128:256])
                ms.append(m)
                pb = e.astype(BF16)
                parts = []
                for k in range(8):
                    parts.append(pb[64 * k : 64 * k + 64, 0:128])
                    parts.append(pb[64 * k : 64 * k + 64, 128:256])
                ps.append(jnp.concatenate(parts, axis=0))
            prod = dot(vals, jnp.concatenate(ps, axis=1))
            mnew = jnp.broadcast_to(jnp.concatenate(ms, axis=1), (8, 256))
            absorb(h, mnew, jnp.concatenate(sums, axis=1), prod)

        @pl.when(it % 4 == 3)
        def _():
            c = bufa[pl.ds(base - 12, 16), 128:144, :].reshape(256, 128)
            cc = jnp.concatenate([c, c], axis=1)
            cvt = c.astype(F32).T[HD:128, :].astype(BF16)
            for h in range(NH):
                s = dot(cc, qctx[h]) + bias[0:1, h : h + 1] * LOG2E
                mold = mst[h]
                m = jnp.maximum(jnp.max(s, axis=0, keepdims=True), mold[0:1, :])
                e = jnp.exp2(s - m)
                r = jnp.sum(e.reshape(32, 8, 256), axis=0)
                prod = dot(cvt, e.astype(BF16))
                absorb(h, jnp.broadcast_to(m, (8, 256)), r, prod)

        return carry

    lax.fori_loop(0, 16, step, 0)

    heads = []
    for h in range(NH):
        total = jnp.sum(lst[h], axis=0, keepdims=True)
        heads.append(acc[h] / total)
    att[x] = jnp.concatenate(heads, axis=0).T.astype(BF16)

    left = lax.rem(x + XN - 1, XN)
    right = lax.rem(x + 1, XN)
    far = lax.rem(x + 2, XN)

    def att_copy(slot, half, sem, k):
        part = att.at[slot, half * 128 : half * 128 + 128]
        return remote(part, part, satt.at[sem], ratt.at[sem], at_x(k))

    own = [att_copy(x, 0, 0, 1), att_copy(x, 1, 1, -1), att_copy(x, 1, 2, 1), att_copy(x, 0, 3, -1)]
    for c in own:
        c.start()
    own[0].wait_recv()
    fwd0 = att_copy(left, 0, 4, 1)
    fwd0.start()
    own[1].wait_recv()
    fwd1 = att_copy(right, 1, 5, -1)
    fwd1.start()
    own[2].wait_recv()
    own[3].wait_recv()
    for s, slot in ((4, left), (5, right), (6, far)):
        remote(wo.at[slot, d], wo.at[slot, d], swo.at[s], rwo.at[s], partner).wait()
    fwd0.wait()
    fwd1.wait()

    gate = vec(ma_x, 8)
    outs = []
    for c in range(8):
        side, off = c // 4, (c % 4) * 256
        mixed = jnp.zeros((TOK, 256), F32)
        for g in range(XN):
            mixed = mixed + dot(att[g], wo[g, side, :, off : off + 256]).astype(BF16).astype(F32)
        cols = slice(c * 256, (c + 1) * 256)
        outv[:, cols] = (lat[:, cols].astype(F32) + gate[:, cols] * mixed).astype(BF16)
        o = pltpu.make_async_copy(outv.at[:, cols], out_h.at[:, cols], osem.at[c])
        o.start()
        outs.append(o)

    for c in own:
        c.wait_send()

    def drain(s, carry):
        remote(bufa.at[s], bufa.at[s], sa.at[s], ra.at[s], at_z(1)).wait_send()
        remote(bufb.at[s], bufb.at[s], sb.at[s], rb.at[s], at_y(1)).wait_send()
        return carry

    lax.fori_loop(1, 64, drain, 0)
    for o in outs:
        o.wait()


def on_device(
    latent, condition, context, context_code, shift_weight, scale_weight, gate_weight, norm_gain,
    query_weight, key_weight, value_weight, output_weight, query_gain, key_gain, context_bias,
):
    V = pltpu.VMEM
    dma = pltpu.SemaphoreType.DMA
    scratch = [
        V((TOK, D), BF16), V((1, 32), BF16), V((CTXT, D), BF16), V((1, 32), BF16),
        V((32, 512), BF16), V((32, 512), BF16), V((32, 512), BF16), V((1, D), F32),
        V((D, QC), BF16), V((D, HD), BF16), V((D, HD), BF16), V((XN, 2, QC, D // 2), BF16),
        V((1, HD), F32), V((1, HD), F32), V((1, NH), F32),
        V((TOK, D), BF16), V((TOK + CTXT, D), BF16), V((D, 128), BF16),
        V((8, 256, 256), BF16), V((NH, 256, 256), BF16),
        V((64, 144, 128), BF16), V((64, 128, 128), BF16),
        V((NH, 8, 256), F32), V((NH, 8, 256), F32), V((NH, HD, 256), F32), V((XN, TOK, QC), BF16),
        V((16, 128), F32), V((RING, 16, 128), F32), V((1, 16, 128), F32), V((RING, 16, 128), F32), V((XN, 16, 128), F32),
        V((8, 128), F32), V((RING, 8, 128), F32), V((1, 8, 128), F32), V((RING, 8, 128), F32), V((XN, 8, 128), F32),
        dma((16,)), dma((8,)), dma((64,)), dma((64,)), dma((64,)), dma((64,)),
        dma((40,)), dma((40,)), dma((8,)), dma((8,)), dma((8,)), dma((8,)),
    ]
    out = pl.pallas_call(
        kernel,
        out_shape=jax.ShapeDtypeStruct((TOK, D), BF16),
        in_specs=[pl.BlockSpec(memory_space=pl.ANY)] * 15,
        out_specs=pl.BlockSpec(memory_space=pl.ANY),
        scratch_shapes=scratch,
        compiler_params=pltpu.CompilerParams(
            collective_id=0, has_side_effects=True, vmem_limit_bytes=60 * 1024 * 1024
        ),
        name="fused",
    )(
        latent[0], condition, context[0], context_code[None], shift_weight, scale_weight, gate_weight,
        norm_gain[None], query_weight, key_weight, value_weight, output_weight,
        query_gain[None], key_gain[None], context_bias[None],
    )
    return out[None]


def solution(mesh):
    return jax.shard_map(
        on_device,
        mesh=mesh,
        in_specs=(
            P("dp", "sp", None), P("dp", "sp"), P("dp", "sp", None), P("sp"),
            P("sp", "tp"), P("sp", "tp"), P("sp", "tp"), P(),
            P(None, "tp"), P(None, "tp"), P(None, "tp"), P("tp", None),
            P(), P(), P("tp"),
        ),
        out_specs=P("dp", "sp", None),
        check_vma=False,
    )
```

```python
import functools
import math

import jax
import jax.numpy as jnp
from jax import lax
from jax.experimental import pallas as pl
from jax.experimental.pallas import tpu as pltpu
from jax.sharding import PartitionSpec as P

MESH = pl.DeviceIdType.MESH
F32 = jnp.float32
BF16 = jnp.bfloat16
EPS = 1e-6
ROPE_BASE = 10000.0
GRID_W = 64
RING = 8
XN = 4
TOK = 256
CTXT = 16
D = 2048
HD = 64
NH = 4
QC = NH * HD
LOG2E = 1.4426950408889634


ORDER = [
    (0, 0), (1, 0), (2, 0), (0, -1), (0, 1), (4, 0), (3, 0), (1, 1), (1, -1), (2, -1), (2, 1), (0, 2), (0, -2),
    (5, 0), (6, 0), (3, -1), (3, 1), (4, -1), (4, 1), (1, 2), (1, -2), (5, -1), (7, 0), (5, 1), (6, -1), (2, -2),
    (6, 1), (3, -2), (2, 2), (7, -1), (7, 1), (4, -2), (3, 2), (5, -2), (4, 2), (6, -2), (5, 2), (7, -2), (6, 2),
    (0, -3), (7, 2), (1, -3), (0, 3), (1, 3), (2, -3), (3, -3), (2, 3), (4, -3), (3, 3), (4, 3), (5, -3), (5, 3),
    (6, -3), (7, -3), (6, 3), (7, 3), (0, 4), (1, 4), (2, 4), (3, 4), (4, 4), (5, 4), (6, 4), (7, 4),
]
SLOT = {item: n for n, item in enumerate(ORDER)}
NEXT = {0: ((1, 1), (2, -1)), 1: ((3, 1),), 2: ((4, -1),), 3: ((5, 1),), 4: ((6, -1),), 5: ((7, 1),)}


def onward(item):
    i, r = item
    out = []
    if r == 0:
        out += [(0, way, SLOT[(j, 0)]) for j, way in NEXT.get(i, ())]
    if 0 <= r < 4:
        out.append((1, 1, SLOT[(i, r + 1)]))
    if -3 < r <= 0:
        out.append((1, -1, SLOT[(i, r - 1)]))
    return out


def dot(a, b):
    return jnp.dot(a, b, preferred_element_type=F32)


def kernel(
    latent_h, cond_h, context_h, code_h, shw_h, scw_h, gaw_h, ngain_h, wq_h, wk_h, wv_h, wo_h, qg_h, kg_h, bias_h,
    out_h,
    lat, cond, ctx, code, shw, scw, gaw, ngain, wq, wkv, wo, qg, kg, bias,
    outv, normed, qbd, qctx, bufa, bufb, mst, alp, lst, acc, att, sbuf0, sbuf1, sctx,
    ma, ma_y, ma_s, ma_z, ma_x, mb, mb_z, mb_s, mb_y, mb_x,
    lsem, osem, sa, ra, sb, rb, smod, rmod, swo, rwo, satt, ratt,
):
    sp = lax.axis_index("sp")
    x = lax.axis_index("tp")
    d = lax.axis_index("dp")
    z = sp // RING
    y = sp % RING
    sgn = 1 - 2 * d

    def at_y(k):
        return {"sp": z * RING + lax.rem(y + k + 2 * RING, RING)}

    def at_z(k):
        return {"sp": lax.rem(z + k + 2 * RING, RING) * RING + y}

    def at_x(k):
        return {"tp": lax.rem(x + k + 2 * XN, XN)}

    partner = {"dp": 1 - d}

    def remote(src, dst, ss, rs, dev):
        return pltpu.make_async_remote_copy(
            src_ref=src, dst_ref=dst, send_sem=ss, recv_sem=rs, device_id=dev, device_id_type=MESH
        )

    pairs = [
        (cond_h, cond), (code_h, code), (shw_h, shw), (scw_h, scw), (gaw_h, gaw),
        (latent_h, lat), (context_h, ctx), (ngain_h, ngain), (wk_h, wkv.at[0:HD]), (wv_h, wkv.at[HD : 2 * HD]), (wq_h, wq),
        (qg_h, qg), (kg_h, kg), (bias_h, bias),
        (wo_h.at[:, 0 : D // 2], wo.at[x, 0]), (wo_h.at[:, D // 2 : D], wo.at[x, 1]),
    ]
    loads = [pltpu.make_async_copy(s, t, lsem.at[i]) for i, (s, t) in enumerate(pairs)]
    for c in loads:
        c.start()

    barrier = pltpu.get_barrier_semaphore()
    for k in range(1, RING):
        pl.semaphore_signal(barrier, inc=1, device_id=at_y(k), device_id_type=MESH)
        pl.semaphore_signal(barrier, inc=1, device_id=at_z(k), device_id_type=MESH)
    for k in range(1, XN):
        pl.semaphore_signal(barrier, inc=1, device_id=at_x(k), device_id_type=MESH)
    pl.semaphore_signal(barrier, inc=1, device_id=partner, device_id_type=MESH)

    for i in range(5):
        loads[i].wait()
    both = jnp.concatenate([cond[...], code[...]], axis=0).astype(F32)
    act = (both * (1.0 / (1.0 + jnp.exp(-both)))).astype(BF16)
    pshift = dot(act, shw[...])
    pscale = dot(act, scw[...])
    pgate = dot(act, gaw[...])
    for c in range(4):
        cols = slice(c * 128, (c + 1) * 128)
        ma[c : c + 1, :] = pshift[0:1, cols]
        ma[4 + c : 5 + c, :] = pscale[0:1, cols]
        ma[8 + c : 9 + c, :] = pgate[0:1, cols]
        mb[c : c + 1, :] = pshift[1:2, cols]
        mb[4 + c : 5 + c, :] = pscale[1:2, cols]
    ma[12:16, :] = jnp.zeros((4, 128), F32)

    pl.semaphore_wait(barrier, 2 * (RING - 1) + (XN - 1) + 1)

    def spread(src, dst, sem, at):
        for k in range(1, RING):
            remote(src, dst.at[k], smod.at[sem], rmod.at[sem], at(k)).start()

    def spread_wait(dst, sem):
        part = dst.at[1:RING]
        remote(part, part, smod.at[sem], rmod.at[sem], at_y(1)).wait()

    spread(ma, ma_y, 0, at_y)
    spread(mb, mb_z, 1, at_z)

    for i in (14, 15):
        loads[i].wait()
    wo1 = [
        remote(wo.at[x, d], wo.at[x, d], swo.at[0], rwo.at[0], at_x(1)),
        remote(wo.at[x, d], wo.at[x, d], swo.at[1], rwo.at[1], at_x(-1)),
    ]
    for c in wo1:
        c.start()

    for i in (5, 6, 7, 8, 9):
        loads[i].wait()
    lf = lat[...].astype(F32)
    rms = lax.rsqrt(jnp.mean(lf * lf, axis=-1, keepdims=True) + EPS)
    cf = ctx[...].astype(F32)
    crms = lax.rsqrt(jnp.mean(cf * cf, axis=-1, keepdims=True) + EPS)
    qbd[...] = jnp.zeros(qbd.shape, BF16)
    qctx[...] = jnp.zeros(qctx.shape, BF16)
    mst[...] = jnp.full(mst.shape, -1e30, F32)
    lst[...] = jnp.zeros(lst.shape, F32)
    acc[...] = jnp.zeros(acc.shape, F32)
    fi = lax.broadcasted_iota(jnp.int32, (32, TOK), 0)
    ti = lax.broadcasted_iota(jnp.int32, (32, TOK), 1)
    grow = sp * (TOK // GRID_W) + ti // GRID_W
    gcol = ti % GRID_W
    gpos = jnp.where(fi < 16, grow, gcol).astype(F32)
    inv = jnp.exp((fi % 16).astype(F32) * (-math.log(ROPE_BASE) / 16.0))
    angle = gpos * inv
    cosv = jnp.cos(angle)
    sinv = jnp.sin(angle)

    spread_wait(ma_y, 0)
    spread_wait(mb_z, 1)
    ta = ma[...]
    tb = mb[...]
    for k in range(1, RING):
        ta = ta + ma_y[k]
        tb = tb + mb_z[k]
    ma_s[0] = ta
    mb_s[0] = tb
    spread(ma_s.at[0], ma_z, 2, at_z)
    spread(mb_s.at[0], mb_y, 3, at_y)
    spread_wait(ma_z, 2)
    spread_wait(mb_y, 3)
    for k in range(1, RING):
        ta = ta + ma_z[k]
        tb = tb + mb_y[k]
    ma_x[x] = ta
    mb_x[x] = tb
    for k in range(1, XN):
        remote(ma_x.at[x], ma_x.at[x], smod.at[4], rmod.at[4], at_x(k)).start()
        remote(mb_x.at[x], mb_x.at[x], smod.at[5], rmod.at[5], at_x(k)).start()
    for ref, sem in ((ma_x, 4), (mb_x, 5)):
        part = ref.at[1:XN]
        remote(part, part, smod.at[sem], rmod.at[sem], at_x(1)).wait()
    def vec(ref, row):
        return jnp.concatenate([ref[i, row + c : row + c + 1, :] for i in range(XN) for c in range(4)], axis=1)

    gain = ngain[...]
    lshift = vec(ma_x, 0)
    lscale = gain * (1.0 + vec(ma_x, 4))
    cshift = vec(mb_x, 0)
    cscale = gain * (1.0 + vec(mb_x, 4))
    normed[0:TOK, :] = (lat[...].astype(F32) * rms * lscale + lshift).astype(BF16)
    normed[TOK : TOK + CTXT, :] = (cf * crms * cscale + cshift).astype(BF16)

    kv = lax.dot_general(normed[...], wkv[...], (((1,), (1,)), ((), ())), preferred_element_type=F32)
    kvt = kv[0:TOK, :].T
    for i in (10, 11, 12, 13):
        loads[i].wait()
    eye = lax.broadcasted_iota(jnp.int32, (HD, HD), 0) == lax.broadcasted_iota(jnp.int32, (HD, HD), 1)
    qgain = jnp.sum(jnp.where(eye, qg[...], 0.0), axis=1, keepdims=True)
    kgain = jnp.sum(jnp.where(eye, kg[...], 0.0), axis=1, keepdims=True)

    def norm_rope(t, g):
        t = t * lax.rsqrt(jnp.mean(t * t, axis=0, keepdims=True) + EPS) * g
        a, b = t[0:32, :], t[32:64, :]
        return jnp.concatenate([a * cosv - b * sinv, b * cosv + a * sinv], axis=0)

    kt = norm_rope(kvt[0:HD, :], kgain)
    k2 = jnp.concatenate([kt, kt], axis=0).T
    low = lax.broadcasted_iota(jnp.int32, (HD, 128), 1) < HD
    vt = kvt[HD : 2 * HD, :].astype(BF16)
    bufa[0, 0:64, :] = jnp.where(low, k2[0:64], k2[64:128]).astype(BF16)
    bufb[0, 0:64, :] = jnp.where(low, k2[128:192], k2[192:256]).astype(BF16)
    bufa[0, 64:128, :] = vt[:, 0:128]
    bufb[0, 64:128, :] = vt[:, 128:256]
    ckv = kv[TOK : TOK + CTXT, :]
    lowc = lax.broadcasted_iota(jnp.int32, (CTXT, 128), 1) < HD
    csq = jnp.sum(jnp.where(lowc, ckv * ckv, 0.0), axis=1, keepdims=True) * (1.0 / HD)
    kg2 = jnp.concatenate([kg[...], kg[...]], axis=1)
    bufa[0, 128:144, :] = jnp.where(lowc, ckv * lax.rsqrt(csq + EPS) * kg2, ckv).astype(BF16)

    def ring(axis, k):
        along_y = 1 - d if axis == 0 else d
        k = k * sgn
        return {
            "sp": lax.rem(z + (1 - along_y) * k + RING, RING) * RING + lax.rem(y + along_y * k + RING, RING)
        }

    def group(s):
        return s if s < 16 else 8 + s // 2

    def pass_on(s):
        for axis, way, t in onward(ORDER[s]):
            remote(bufa.at[s], bufa.at[t], sa, ra.at[group(t)], ring(axis, way)).start()
            remote(bufb.at[s], bufb.at[t], sb, rb.at[group(t)], ring(1 - axis, way)).start()

    def arrived(s, n):
        pa, pb = bufa.at[s : s + n], bufb.at[s : s + n]
        remote(pa, pa, sa, ra.at[group(s)], at_z(1)).wait_recv()
        remote(pb, pb, sb, rb.at[group(s)], at_y(1)).wait_recv()

    pass_on(0)

    q = dot(normed[0:TOK, :], wq[...])
    qt = q.T
    for h in range(NH):
        qh = norm_rope(qt[h * HD : (h + 1) * HD, :], qgain).astype(BF16)
        qs = qh.astype(F32) * (LOG2E * HD**-0.5)
        hi = qs.astype(BF16)
        lo = (qs - hi.astype(F32)).astype(BF16)
        for t in range(2):
            cols = slice(t * 128, (t + 1) * 128)
            for r, part in ((0, hi), (128, lo)):
                qbd[2 * h + t, r : r + 64, 0:128] = part[:, cols]
                qbd[2 * h + t, r + 64 : r + 128, 128:256] = part[:, cols]
        qctx[h, 0:64, :] = hi
        qctx[h, 128:192, :] = lo

    sbuf = (sbuf0, sbuf1)

    def keep(keys, h, sref):
        for t in range(2):
            sc = dot(keys, qbd[2 * h + t])
            sref[:, :, t * 256 : (t + 1) * 256] = sc.reshape(4, 128, 256)
            m = jnp.max(sc.reshape(64, 8, 256), axis=0)
            m = jnp.maximum(m[:, 0:128], m[:, 128:256])
            cols = slice(t * 128, (t + 1) * 128)
            mold = mst[h, :, cols]
            m = jnp.maximum(jnp.broadcast_to(jnp.max(m, axis=0, keepdims=True), (8, 128)), mold)
            mst[h, :, cols] = m
            alp[h, :, cols] = jnp.exp2(mold - m)

    def use(vals, h, sref, zero):
        m = jnp.concatenate([mst[h, :, 0:128]] * 2 + [mst[h, :, 128:256]] * 2, axis=1)
        alpha = alp[h]
        rows = jnp.zeros((8, 512), F32)
        prod = jnp.zeros((HD, 256), F32)
        for k in range(4):
            e = jnp.exp2(sref[k + zero].reshape(16, 8, 512) - m[None])
            rows = rows + jnp.sum(e, axis=0)
            pb = e.reshape(128, 512).astype(BF16)
            p = jnp.concatenate(
                [
                    jnp.concatenate([pb[r : r + 64, c : c + 128], pb[r : r + 64, c + 256 : c + 384]], axis=1)
                    for r in (0, 64)
                    for c in (0, 128)
                ],
                axis=0,
            )
            prod = prod + dot(vals[:, 256 * k : 256 * k + 256], p)
        rows = jnp.concatenate([rows[:, 0:128] + rows[:, 128:256], rows[:, 256:384] + rows[:, 384:512]], axis=1)
        alp[h] = jnp.ones((8, 256), F32)
        lst[h] = lst[h] * alpha + rows
        acc[h] = acc[h] * alpha[0:1, :] + prod

    def receive(st):
        n = 1 if st < 4 else 2
        for s in range(4 * st, 4 * st + 4, n):
            if s > 0:
                arrived(s, n)
                for t in range(n):
                    pass_on(s + t)

    def pick(value, low, high):
        if high - low == 1:
            receive(low)
            return
        mid = (low + high) // 2

        @pl.when(value < mid)
        def _():
            pick(value, low, mid)

        @pl.when(value >= mid)
        def _():
            pick(value, mid, high)

    def keys_of(base):
        k = jnp.concatenate(
            [bufa[pl.ds(base, 4), 0:64, :].reshape(256, 128), bufb[pl.ds(base, 4), 0:64, :].reshape(256, 128)], axis=0
        )
        return jnp.concatenate([k, k], axis=1)

    def step(it, carry):
        base = it * 4
        zero = jnp.minimum(it, 0)

        pick(it, 0, 16)

        @pl.when(it == 8)
        def _():
            for c in wo1:
                c.wait()
            left = lax.rem(x + XN - 1, XN)
            right = lax.rem(x + 1, XN)
            remote(wo.at[left, d, 0:128], wo.at[left, d, 0:128], swo.at[2], rwo.at[2], at_x(1)).start()
            remote(wo.at[right, d, 128:256], wo.at[right, d, 128:256], swo.at[3], rwo.at[3], at_x(-1)).start()
            remote(wo.at[left, d], wo.at[left, d], swo.at[4], rwo.at[4], partner).start()
            remote(wo.at[right, d], wo.at[right, d], swo.at[5], rwo.at[5], partner).start()

        @pl.when(it == 14)
        def _():
            far = lax.rem(x + 2, XN)
            remote(wo.at[far, d, 0:128], wo.at[far, d, 0:128], swo.at[2], rwo.at[2], at_x(1)).wait()
            remote(wo.at[far, d, 128:256], wo.at[far, d, 128:256], swo.at[3], rwo.at[3], at_x(-1)).wait()
            remote(wo.at[far, d], wo.at[far, d], swo.at[6], rwo.at[6], partner).start()

        keys = keys_of(base)
        vals = jnp.concatenate(
            [bufa[base + k, 64:128, :] for k in range(4)] + [bufb[base + k, 64:128, :] for k in range(4)], axis=1
        )
        keep(keys, 0, sbuf[0])
        for h in range(NH):
            if h + 1 < NH:
                keep(keys, h + 1, sbuf[(h + 1) % 2])
            use(vals, h, sbuf[h % 2], zero)

        @pl.when(it % 4 == 3)
        def _():
            c = bufa[pl.ds(base - 12, 16), 128:144, :].reshape(256, 128)
            cc = jnp.concatenate([c, c], axis=1)
            cvt = c.astype(F32).T[HD:128, :].astype(BF16)
            for h in range(NH):
                sc = dot(cc, qctx[h]) + bias[0:1, h : h + 1] * LOG2E
                sctx[h] = sc
                m = jnp.max(sc.reshape(32, 8, 256), axis=0)
                mold = mst[h]
                m = jnp.maximum(jnp.broadcast_to(jnp.max(m, axis=0, keepdims=True), (8, 256)), mold)
                mst[h] = m
                alp[h] = alp[h] * jnp.exp2(mold - m)
            for h in range(NH):
                alpha = alp[h]
                alp[h] = jnp.ones((8, 256), F32)
                e = jnp.exp2(sctx[h + zero].reshape(32, 8, 256) - mst[h][None])
                prod = dot(cvt, e.reshape(256, 256).astype(BF16))
                lst[h] = lst[h] * alpha + jnp.sum(e, axis=0)
                acc[h] = acc[h] * alpha[0:1, :] + prod

        return carry

    lax.fori_loop(0, 16, step, 0)

    heads = []
    for h in range(NH):
        total = jnp.sum(lst[h], axis=0, keepdims=True)
        heads.append(acc[h] / total)
    att[x] = jnp.concatenate(heads, axis=0).T.astype(BF16)

    left = lax.rem(x + XN - 1, XN)
    right = lax.rem(x + 1, XN)
    far = lax.rem(x + 2, XN)

    def att_copy(slot, half, sem, k):
        part = att.at[slot, half * 128 : half * 128 + 128]
        return remote(part, part, satt.at[sem], ratt.at[sem], at_x(k))

    own = [att_copy(x, 0, 0, 1), att_copy(x, 1, 1, -1), att_copy(x, 1, 2, 1), att_copy(x, 0, 3, -1)]
    for c in own:
        c.start()
    pa, pb = bufa.at[1:64], bufb.at[1:64]
    remote(pa, pa, sa, ra.at[0], at_z(1)).wait_send()
    remote(pb, pb, sb, rb.at[0], at_y(1)).wait_send()
    own[0].wait_recv()
    fwd0 = att_copy(left, 0, 4, 1)
    fwd0.start()
    own[1].wait_recv()
    fwd1 = att_copy(right, 1, 5, -1)
    fwd1.start()
    own[2].wait_recv()
    own[3].wait_recv()
    for s, slot in ((4, left), (5, right), (6, far)):
        remote(wo.at[slot, d], wo.at[slot, d], swo.at[s], rwo.at[s], partner).wait()
    fwd0.wait()
    fwd1.wait()

    gate = vec(ma_x, 8)
    outs = []
    for c in range(8):
        side, off = c // 4, (c % 4) * 256
        mixed = jnp.zeros((TOK, 256), F32)
        for g in range(XN):
            mixed = mixed + dot(att[g], wo[g, side, :, off : off + 256]).astype(BF16).astype(F32)
        cols = slice(c * 256, (c + 1) * 256)
        outv[:, cols] = (lat[:, cols].astype(F32) + gate[:, cols] * mixed).astype(BF16)
        o = pltpu.make_async_copy(outv.at[:, cols], out_h.at[:, cols], osem.at[c])
        o.start()
        outs.append(o)

    for c in own:
        c.wait_send()

    for o in outs:
        o.wait()


def on_device(
    latent, condition, context, context_code, shift_weight, scale_weight, gate_weight, norm_gain,
    query_weight, key_weight, value_weight, output_weight, query_gain, key_gain, context_bias,
):
    V = pltpu.VMEM
    dma = pltpu.SemaphoreType.DMA
    scratch = [
        V((TOK, D), BF16), V((1, 32), BF16), V((CTXT, D), BF16), V((1, 32), BF16),
        V((32, 512), BF16), V((32, 512), BF16), V((32, 512), BF16), V((1, D), F32),
        V((D, QC), BF16), V((2 * HD, D), BF16), V((XN, 2, QC, D // 2), BF16),
        V((1, HD), F32), V((1, HD), F32), V((1, NH), F32),
        V((TOK, D), BF16), V((TOK + CTXT, D), BF16),
        V((8, 256, 256), BF16), V((NH, 256, 256), BF16),
        V((64, 144, 128), BF16), V((64, 128, 128), BF16),
        V((NH, 8, 256), F32), V((NH, 8, 256), F32), V((NH, 8, 256), F32), V((NH, HD, 256), F32), V((XN, TOK, QC), BF16),
        V((4, 128, 512), F32), V((4, 128, 512), F32), V((NH, 256, 256), F32),
        V((16, 128), F32), V((RING, 16, 128), F32), V((1, 16, 128), F32), V((RING, 16, 128), F32), V((XN, 16, 128), F32),
        V((8, 128), F32), V((RING, 8, 128), F32), V((1, 8, 128), F32), V((RING, 8, 128), F32), V((XN, 8, 128), F32),
        dma((16,)), dma((8,)), dma, dma((40,)), dma, dma((40,)),
        dma((6,)), dma((6,)), dma((7,)), dma((7,)), dma((6,)), dma((6,)),
    ]
    out = pl.pallas_call(
        kernel,
        out_shape=jax.ShapeDtypeStruct((TOK, D), BF16),
        in_specs=[pl.BlockSpec(memory_space=pl.ANY)] * 15,
        out_specs=pl.BlockSpec(memory_space=pl.ANY),
        scratch_shapes=scratch,
        compiler_params=pltpu.CompilerParams(
            collective_id=0, has_side_effects=True, vmem_limit_bytes=60 * 1024 * 1024
        ),
        name="fused",
    )(
        latent[0], condition, context[0], context_code[None], shift_weight, scale_weight, gate_weight,
        norm_gain[None], query_weight, key_weight.T, value_weight.T, output_weight,
        query_gain[None], key_gain[None], context_bias[None],
    )
    return out[None]


def solution(mesh):
    return jax.shard_map(
        on_device,
        mesh=mesh,
        in_specs=(
            P("dp", "sp", None), P("dp", "sp"), P("dp", "sp", None), P("sp"),
            P("sp", "tp"), P("sp", "tp"), P("sp", "tp"), P(),
            P(None, "tp"), P(None, "tp"), P(None, "tp"), P("tp", None),
            P(), P(), P("tp"),
        ),
        out_specs=P("dp", "sp", None),
        check_vma=False,
    )
```

```python
import functools
import math

import jax
import jax.numpy as jnp
from jax import lax
from jax.experimental import pallas as pl
from jax.experimental.pallas import tpu as pltpu
from jax.sharding import PartitionSpec as P

MESH = pl.DeviceIdType.MESH
F32 = jnp.float32
BF16 = jnp.bfloat16
EPS = 1e-6
ROPE_BASE = 10000.0
GRID_W = 64
RING = 8
XN = 4
TOK = 256
CTXT = 16
D = 2048
HD = 64
NH = 4
QC = NH * HD
LOG2E = 1.4426950408889634


ORDER = [
    (0, 0), (2, 0), (1, 0), (0, -1), (0, 1), (4, 0), (2, -1), (3, 0), (2, 1), (1, 1), (1, -1), (0, -2), (5, 0),
    (6, 0), (4, -1), (4, 1), (3, -1), (2, -2), (3, 1), (0, 2), (7, 0), (1, 2), (1, -2), (0, -3), (6, 1), (5, 1),
    (6, -1), (2, 2), (4, -2), (5, -1), (3, -2), (4, 2), (1, -3), (2, -3), (7, 1), (7, -1), (6, 2), (0, 3),
    (6, -2), (3, 2), (5, 2), (4, -3), (1, 3), (2, 3), (7, -2), (7, 2), (5, -2), (4, 3), (3, 3), (6, -3), (6, 3),
    (5, 3), (7, 3), (7, -3), (0, 4), (1, 4), (4, 4), (2, 4), (3, -3), (3, 4), (6, 4), (5, 4), (7, 4), (5, -3),
]
SLOT = {item: n for n, item in enumerate(ORDER)}
NEXT = {0: ((1, 1), (2, -1)), 1: ((3, 1),), 2: ((4, -1),), 3: ((5, 1),), 4: ((6, -1),), 5: ((7, 1),)}


def onward(item):
    i, r = item
    out = []
    if r == 0:
        out += [(0, way, SLOT[(j, 0)]) for j, way in NEXT.get(i, ())]
    if 0 <= r < 4:
        out.append((1, 1, SLOT[(i, r + 1)]))
    if -3 < r <= 0:
        out.append((1, -1, SLOT[(i, r - 1)]))
    return out


def dot(a, b):
    return jnp.dot(a, b, preferred_element_type=F32)


def kernel(
    latent_h, cond_h, context_h, code_h, shw_h, scw_h, gaw_h, ngain_h, wq_h, wk_h, wv_h, wo_h, qg_h, kg_h, bias_h,
    out_h,
    lat, cond, ctx, code, shw, scw, gaw, ngain, wq, wkv, wo, qg, kg, bias,
    outv, normed, qbd, qctx, bufa, bufb, mst, alp, acc, att, sbuf0, sbuf1, sctx,
    ma, ma_y, ma_s, ma_z, ma_x, mg, mg_y, mg_s, mg_z, mg_x, mb, mb_z, mb_s, mb_y, mb_x,
    lsem, osem, sa, ra, sb, rb, smod, rmod, swo, rwo, satt, ratt,
):
    sp = lax.axis_index("sp")
    x = lax.axis_index("tp")
    d = lax.axis_index("dp")
    z = sp // RING
    y = sp % RING
    sgn = 1 - 2 * d

    def at_y(k):
        return {"sp": z * RING + lax.rem(y + k + 2 * RING, RING)}

    def at_z(k):
        return {"sp": lax.rem(z + k + 2 * RING, RING) * RING + y}

    def at_x(k):
        return {"tp": lax.rem(x + k + 2 * XN, XN)}

    partner = {"dp": 1 - d}

    def remote(src, dst, ss, rs, dev):
        return pltpu.make_async_remote_copy(
            src_ref=src, dst_ref=dst, send_sem=ss, recv_sem=rs, device_id=dev, device_id_type=MESH
        )

    pairs = [
        (cond_h, cond), (code_h, code), (shw_h, shw), (scw_h, scw), (gaw_h, gaw),
        (latent_h, lat), (context_h, ctx), (ngain_h, ngain), (wk_h, wkv.at[0:HD]), (wv_h, wkv.at[HD : 2 * HD]), (wq_h, wq),
        (qg_h, qg), (kg_h, kg), (bias_h, bias),
        (wo_h.at[:, 0 : D // 2], wo.at[x, 0]), (wo_h.at[:, D // 2 : D], wo.at[x, 1]),
    ]
    loads = [pltpu.make_async_copy(s, t, lsem.at[i]) for i, (s, t) in enumerate(pairs)]
    for c in loads:
        c.start()

    barrier = pltpu.get_barrier_semaphore()
    for k in range(1, RING):
        pl.semaphore_signal(barrier, inc=1, device_id=at_y(k), device_id_type=MESH)
        pl.semaphore_signal(barrier, inc=1, device_id=at_z(k), device_id_type=MESH)
    for k in range(1, XN):
        pl.semaphore_signal(barrier, inc=1, device_id=at_x(k), device_id_type=MESH)
    pl.semaphore_signal(barrier, inc=1, device_id=partner, device_id_type=MESH)

    for i in range(5):
        loads[i].wait()
    both = jnp.concatenate([cond[...], code[...]], axis=0).astype(F32)
    act = (both * (1.0 / (1.0 + jnp.exp(-both)))).astype(BF16)
    pshift = dot(act, shw[...])
    pscale = dot(act, scw[...])
    pgate = dot(act, gaw[...])
    for c in range(4):
        cols = slice(c * 128, (c + 1) * 128)
        ma[c : c + 1, :] = pshift[0:1, cols]
        ma[4 + c : 5 + c, :] = pscale[0:1, cols]
        mg[c : c + 1, :] = pgate[0:1, cols]
        mb[c : c + 1, :] = pshift[1:2, cols]
        mb[4 + c : 5 + c, :] = pscale[1:2, cols]
    mg[4:8, :] = jnp.zeros((4, 128), F32)

    pl.semaphore_wait(barrier, 2 * (RING - 1) + (XN - 1) + 1)

    def spread(src, dst, sem, at):
        for k in range(1, RING):
            remote(src, dst.at[k], smod.at[sem], rmod.at[sem], at(k)).start()

    def spread_wait(dst, sem):
        part = dst.at[1:RING]
        remote(part, part, smod.at[sem], rmod.at[sem], at_y(1)).wait()

    spread(ma, ma_y, 0, at_y)
    spread(mb, mb_z, 1, at_z)

    for i in (5, 6, 7, 8, 9):
        loads[i].wait()
    lf = lat[...].astype(F32)
    rms = lax.rsqrt(jnp.mean(lf * lf, axis=-1, keepdims=True) + EPS)
    cf = ctx[...].astype(F32)
    crms = lax.rsqrt(jnp.mean(cf * cf, axis=-1, keepdims=True) + EPS)
    qbd[...] = jnp.zeros(qbd.shape, BF16)
    qctx[...] = jnp.zeros(qctx.shape, BF16)
    mst[...] = jnp.full(mst.shape, -1e30, F32)
    acc[...] = jnp.zeros(acc.shape, F32)
    fi = lax.broadcasted_iota(jnp.int32, (32, TOK), 0)
    ti = lax.broadcasted_iota(jnp.int32, (32, TOK), 1)
    grow = sp * (TOK // GRID_W) + ti // GRID_W
    gcol = ti % GRID_W
    gpos = jnp.where(fi < 16, grow, gcol).astype(F32)
    inv = jnp.exp((fi % 16).astype(F32) * (-math.log(ROPE_BASE) / 16.0))
    angle = gpos * inv
    cosv = jnp.cos(angle)
    sinv = jnp.sin(angle)

    spread_wait(ma_y, 0)
    spread_wait(mb_z, 1)
    ta = ma[...]
    tb = mb[...]
    for k in range(1, RING):
        ta = ta + ma_y[k]
        tb = tb + mb_z[k]
    ma_s[0] = ta
    mb_s[0] = tb
    spread(ma_s.at[0], ma_z, 2, at_z)
    spread(mb_s.at[0], mb_y, 3, at_y)
    spread_wait(ma_z, 2)
    spread_wait(mb_y, 3)
    for k in range(1, RING):
        ta = ta + ma_z[k]
        tb = tb + mb_y[k]
    ma_x[x] = ta
    mb_x[x] = tb
    for k in range(1, XN):
        remote(ma_x.at[x], ma_x.at[x], smod.at[4], rmod.at[4], at_x(k)).start()
        remote(mb_x.at[x], mb_x.at[x], smod.at[5], rmod.at[5], at_x(k)).start()
    for ref, sem in ((ma_x, 4), (mb_x, 5)):
        part = ref.at[1:XN]
        remote(part, part, smod.at[sem], rmod.at[sem], at_x(1)).wait()
    def vec(ref, row):
        return jnp.concatenate([ref[i, row + c : row + c + 1, :] for i in range(XN) for c in range(4)], axis=1)

    gain = ngain[...]
    lshift = vec(ma_x, 0)
    lscale = gain * (1.0 + vec(ma_x, 4))
    cshift = vec(mb_x, 0)
    cscale = gain * (1.0 + vec(mb_x, 4))
    normed[0:TOK, :] = (lat[...].astype(F32) * rms * lscale + lshift).astype(BF16)
    normed[TOK : TOK + CTXT, :] = (cf * crms * cscale + cshift).astype(BF16)

    kv = lax.dot_general(normed[...], wkv[...], (((1,), (1,)), ((), ())), preferred_element_type=F32)
    kvt = kv[0:TOK, :].T
    for i in (10, 11, 12, 13):
        loads[i].wait()
    eye = lax.broadcasted_iota(jnp.int32, (HD, HD), 0) == lax.broadcasted_iota(jnp.int32, (HD, HD), 1)
    qgain = jnp.sum(jnp.where(eye, qg[...], 0.0), axis=1, keepdims=True)
    kgain = jnp.sum(jnp.where(eye, kg[...], 0.0), axis=1, keepdims=True)

    def norm_rope(t, g):
        t = t * lax.rsqrt(jnp.mean(t * t, axis=0, keepdims=True) + EPS) * g
        a, b = t[0:32, :], t[32:64, :]
        return jnp.concatenate([a * cosv - b * sinv, b * cosv + a * sinv], axis=0)

    kt = norm_rope(kvt[0:HD, :], kgain)
    k2 = jnp.concatenate([kt, kt], axis=0).T
    low = lax.broadcasted_iota(jnp.int32, (HD, 128), 1) < HD
    vt = kvt[HD : 2 * HD, :].astype(BF16)
    bufa[0, 0:64, :] = jnp.where(low, k2[0:64], k2[64:128]).astype(BF16)
    bufb[0, 0:64, :] = jnp.where(low, k2[128:192], k2[192:256]).astype(BF16)
    bufa[0, 64:128, :] = vt[:, 0:128]
    bufb[0, 64:128, :] = vt[:, 128:256]
    ckv = kv[TOK : TOK + CTXT, :]
    lowc = lax.broadcasted_iota(jnp.int32, (CTXT, 128), 1) < HD
    csq = jnp.sum(jnp.where(lowc, ckv * ckv, 0.0), axis=1, keepdims=True) * (1.0 / HD)
    kg2 = jnp.concatenate([kg[...], kg[...]], axis=1)
    bufa[0, 128:144, :] = jnp.where(lowc, ckv * lax.rsqrt(csq + EPS) * kg2, ckv).astype(BF16)

    def ring(axis, k):
        along_y = 1 - d if axis == 0 else d
        k = k * sgn
        return {
            "sp": lax.rem(z + (1 - along_y) * k + RING, RING) * RING + lax.rem(y + along_y * k + RING, RING)
        }

    def group(s):
        return s if s < 16 else 8 + s // 2

    def pass_on(s):
        for axis, way, t in onward(ORDER[s]):
            remote(bufa.at[s], bufa.at[t], sa, ra.at[group(t)], ring(axis, way)).start()
            remote(bufb.at[s], bufb.at[t], sb, rb.at[group(t)], ring(1 - axis, way)).start()

    def arrived(s, n):
        pa, pb = bufa.at[s : s + n], bufb.at[s : s + n]
        remote(pa, pa, sa, ra.at[group(s)], at_z(1)).wait_recv()
        remote(pb, pb, sb, rb.at[group(s)], at_y(1)).wait_recv()

    pass_on(0)
    spread(mg, mg_y, 6, at_y)
    for i in (14, 15):
        loads[i].wait()
    wo1 = [
        remote(wo.at[x, d], wo.at[x, d], swo.at[0], rwo.at[0], at_x(1)),
        remote(wo.at[x, d], wo.at[x, d], swo.at[1], rwo.at[1], at_x(-1)),
    ]
    for c in wo1:
        c.start()


    q = dot(normed[0:TOK, :], wq[...])
    qt = q.T
    for h in range(NH):
        qh = norm_rope(qt[h * HD : (h + 1) * HD, :], qgain).astype(BF16)
        qs = qh.astype(F32) * (LOG2E * HD**-0.5)
        hi = qs.astype(BF16)
        lo = (qs - hi.astype(F32)).astype(BF16)
        for t in range(2):
            cols = slice(t * 128, (t + 1) * 128)
            for r, part in ((0, hi), (128, lo)):
                qbd[2 * h + t, r : r + 64, 0:128] = part[:, cols]
                qbd[2 * h + t, r + 64 : r + 128, 128:256] = part[:, cols]
        qctx[h, 0:64, :] = hi
        qctx[h, 128:192, :] = lo

    sbuf = (sbuf0, sbuf1)

    def keep(keys, h, sref):
        for t in range(2):
            sc = dot(keys, qbd[2 * h + t])
            sref[:, :, t * 256 : (t + 1) * 256] = sc.reshape(4, 128, 256)
            m = jnp.max(sc.reshape(64, 8, 256), axis=0)
            m = jnp.maximum(m[:, 0:128], m[:, 128:256])
            cols = slice(t * 128, (t + 1) * 128)
            mold = mst[h, :, cols]
            m = jnp.maximum(jnp.broadcast_to(jnp.max(m, axis=0, keepdims=True), (8, 128)), mold)
            mst[h, :, cols] = m
            alp[h, :, cols] = jnp.exp2(mold - m)

    def use(vals, h, sref, zero):
        m = jnp.concatenate([mst[h, :, 0:128]] * 2 + [mst[h, :, 128:256]] * 2, axis=1)
        alpha = alp[h]
        prod = jnp.zeros((HD + 16, 256), F32)
        for k in range(4):
            e = jnp.exp2(sref[k + zero].reshape(16, 8, 512) - m[None])
            pb = e.reshape(128, 512).astype(BF16)
            p = jnp.concatenate(
                [
                    jnp.concatenate([pb[r : r + 64, c : c + 128], pb[r : r + 64, c + 256 : c + 384]], axis=1)
                    for r in (0, 64)
                    for c in (0, 128)
                ],
                axis=0,
            )
            prod = prod + dot(vals[:, 256 * k : 256 * k + 256], p)
        alp[h] = jnp.ones((8, 256), F32)
        acc[h] = acc[h] * alpha[0:1, :] + prod

    def receive(st):
        n = 1 if st < 4 else 2
        for s in range(4 * st, 4 * st + 4, n):
            if s > 0:
                arrived(s, n)
                for t in range(n):
                    pass_on(s + t)

    def pick(value, low, high):
        if high - low == 1:
            receive(low)
            return
        mid = (low + high) // 2

        @pl.when(value < mid)
        def _():
            pick(value, low, mid)

        @pl.when(value >= mid)
        def _():
            pick(value, mid, high)

    def keys_of(base):
        k = jnp.concatenate(
            [bufa[pl.ds(base, 4), 0:64, :].reshape(256, 128), bufb[pl.ds(base, 4), 0:64, :].reshape(256, 128)], axis=0
        )
        return jnp.concatenate([k, k], axis=1)

    def step(it, carry):
        base = it * 4
        zero = jnp.minimum(it, 0)

        pick(it, 0, 16)

        @pl.when(it == 5)
        def _():
            spread_wait(mg_y, 6)
            tg = mg[...]
            for k in range(1, RING):
                tg = tg + mg_y[k]
            mg_s[0] = tg
            spread(mg_s.at[0], mg_z, 7, at_z)

        @pl.when(it == 12)
        def _():
            spread_wait(mg_z, 7)
            tg = mg_s[0]
            for k in range(1, RING):
                tg = tg + mg_z[k]
            mg_x[x] = tg
            for k in range(1, XN):
                remote(mg_x.at[x], mg_x.at[x], smod.at[8], rmod.at[8], at_x(k)).start()

        @pl.when(it == 8)
        def _():
            for c in wo1:
                c.wait()
            left = lax.rem(x + XN - 1, XN)
            right = lax.rem(x + 1, XN)
            remote(wo.at[left, d, 0:128], wo.at[left, d, 0:128], swo.at[2], rwo.at[2], at_x(1)).start()
            remote(wo.at[right, d, 128:256], wo.at[right, d, 128:256], swo.at[3], rwo.at[3], at_x(-1)).start()
            remote(wo.at[left, d], wo.at[left, d], swo.at[4], rwo.at[4], partner).start()
            remote(wo.at[right, d], wo.at[right, d], swo.at[5], rwo.at[5], partner).start()

        @pl.when(it == 14)
        def _():
            far = lax.rem(x + 2, XN)
            remote(wo.at[far, d, 0:128], wo.at[far, d, 0:128], swo.at[2], rwo.at[2], at_x(1)).wait()
            remote(wo.at[far, d, 128:256], wo.at[far, d, 128:256], swo.at[3], rwo.at[3], at_x(-1)).wait()
            remote(wo.at[far, d], wo.at[far, d], swo.at[6], rwo.at[6], partner).start()

        keys = keys_of(base)
        vals = jnp.concatenate(
            [bufa[base + k, 64:128, :] for k in range(4)] + [bufb[base + k, 64:128, :] for k in range(4)], axis=1
        )
        vals = jnp.concatenate([vals, jnp.ones((16, 1024), BF16)], axis=0)
        keep(keys, 0, sbuf[0])
        for h in range(NH):
            if h + 1 < NH:
                keep(keys, h + 1, sbuf[(h + 1) % 2])
            use(vals, h, sbuf[h % 2], zero)

        @pl.when(it % 4 == 3)
        def _():
            c = bufa[pl.ds(base - 12, 16), 128:144, :].reshape(256, 128)
            cc = jnp.concatenate([c, c], axis=1)
            cvt = jnp.concatenate([c.astype(F32).T[HD:128, :].astype(BF16), jnp.ones((16, 256), BF16)], axis=0)
            for h in range(NH):
                sc = dot(cc, qctx[h]) + bias[0:1, h : h + 1] * LOG2E
                sctx[h] = sc
                m = jnp.max(sc.reshape(32, 8, 256), axis=0)
                mold = mst[h]
                m = jnp.maximum(jnp.broadcast_to(jnp.max(m, axis=0, keepdims=True), (8, 256)), mold)
                mst[h] = m
                alp[h] = alp[h] * jnp.exp2(mold - m)
            for h in range(NH):
                alpha = alp[h]
                alp[h] = jnp.ones((8, 256), F32)
                e = jnp.exp2(sctx[h + zero].reshape(32, 8, 256) - mst[h][None])
                prod = dot(cvt, e.reshape(256, 256).astype(BF16))
                acc[h] = acc[h] * alpha[0:1, :] + prod

        return carry

    lax.fori_loop(0, 16, step, 0)

    heads = []
    for h in range(NH):
        heads.append(acc[h, 0:HD] / acc[h, HD : HD + 1])
    att[x] = jnp.concatenate(heads, axis=0).T.astype(BF16)

    left = lax.rem(x + XN - 1, XN)
    right = lax.rem(x + 1, XN)
    far = lax.rem(x + 2, XN)

    def att_copy(slot, half, sem, k):
        part = att.at[slot, half * 128 : half * 128 + 128]
        return remote(part, part, satt.at[sem], ratt.at[sem], at_x(k))

    own = [att_copy(x, 0, 0, 1), att_copy(x, 1, 1, -1), att_copy(x, 1, 2, 1), att_copy(x, 0, 3, -1)]
    for c in own:
        c.start()
    pa, pb = bufa.at[1:64], bufb.at[1:64]
    remote(pa, pa, sa, ra.at[0], at_z(1)).wait_send()
    remote(pb, pb, sb, rb.at[0], at_y(1)).wait_send()
    own[0].wait_recv()
    fwd0 = att_copy(left, 0, 4, 1)
    fwd0.start()
    own[1].wait_recv()
    fwd1 = att_copy(right, 1, 5, -1)
    fwd1.start()
    own[2].wait_recv()
    own[3].wait_recv()
    for s, slot in ((4, left), (5, right), (6, far)):
        remote(wo.at[slot, d], wo.at[slot, d], swo.at[s], rwo.at[s], partner).wait()
    fwd0.wait()
    fwd1.wait()

    piece = mg_x.at[1:XN]
    remote(piece, piece, smod.at[8], rmod.at[8], at_x(1)).wait()
    gate = vec(mg_x, 0)
    outs = []
    for c in range(8):
        side, off = c // 4, (c % 4) * 256
        mixed = jnp.zeros((TOK, 256), F32)
        for g in range(XN):
            mixed = mixed + dot(att[g], wo[g, side, :, off : off + 256]).astype(BF16).astype(F32)
        cols = slice(c * 256, (c + 1) * 256)
        outv[:, cols] = (lat[:, cols].astype(F32) + gate[:, cols] * mixed).astype(BF16)
        o = pltpu.make_async_copy(outv.at[:, cols], out_h.at[:, cols], osem.at[c])
        o.start()
        outs.append(o)

    for c in own:
        c.wait_send()

    for o in outs:
        o.wait()


def on_device(
    latent, condition, context, context_code, shift_weight, scale_weight, gate_weight, norm_gain,
    query_weight, key_weight, value_weight, output_weight, query_gain, key_gain, context_bias,
):
    V = pltpu.VMEM
    dma = pltpu.SemaphoreType.DMA
    scratch = [
        V((TOK, D), BF16), V((1, 32), BF16), V((CTXT, D), BF16), V((1, 32), BF16),
        V((32, 512), BF16), V((32, 512), BF16), V((32, 512), BF16), V((1, D), F32),
        V((D, QC), BF16), V((2 * HD, D), BF16), V((XN, 2, QC, D // 2), BF16),
        V((1, HD), F32), V((1, HD), F32), V((1, NH), F32),
        V((TOK, D), BF16), V((TOK + CTXT, D), BF16),
        V((8, 256, 256), BF16), V((NH, 256, 256), BF16),
        V((64, 144, 128), BF16), V((64, 128, 128), BF16),
        V((NH, 8, 256), F32), V((NH, 8, 256), F32), V((NH, HD + 16, 256), F32), V((XN, TOK, QC), BF16),
        V((4, 128, 512), F32), V((4, 128, 512), F32), V((NH, 256, 256), F32),
        V((8, 128), F32), V((RING, 8, 128), F32), V((1, 8, 128), F32), V((RING, 8, 128), F32), V((XN, 8, 128), F32),
        V((8, 128), F32), V((RING, 8, 128), F32), V((1, 8, 128), F32), V((RING, 8, 128), F32), V((XN, 8, 128), F32),
        V((8, 128), F32), V((RING, 8, 128), F32), V((1, 8, 128), F32), V((RING, 8, 128), F32), V((XN, 8, 128), F32),
        dma((16,)), dma((8,)), dma, dma((40,)), dma, dma((40,)),
        dma((9,)), dma((9,)), dma((7,)), dma((7,)), dma((6,)), dma((6,)),
    ]
    out = pl.pallas_call(
        kernel,
        out_shape=jax.ShapeDtypeStruct((TOK, D), BF16),
        in_specs=[pl.BlockSpec(memory_space=pl.ANY)] * 15,
        out_specs=pl.BlockSpec(memory_space=pl.ANY),
        scratch_shapes=scratch,
        compiler_params=pltpu.CompilerParams(
            collective_id=0, has_side_effects=True, vmem_limit_bytes=60 * 1024 * 1024
        ),
        name="fused",
    )(
        latent[0], condition, context[0], context_code[None], shift_weight, scale_weight, gate_weight,
        norm_gain[None], query_weight, key_weight.T, value_weight.T, output_weight,
        query_gain[None], key_gain[None], context_bias[None],
    )
    return out[None]


def solution(mesh):
    return jax.shard_map(
        on_device,
        mesh=mesh,
        in_specs=(
            P("dp", "sp", None), P("dp", "sp"), P("dp", "sp", None), P("sp"),
            P("sp", "tp"), P("sp", "tp"), P("sp", "tp"), P(),
            P(None, "tp"), P(None, "tp"), P(None, "tp"), P("tp", None),
            P(), P(), P("tp"),
        ),
        out_specs=P("dp", "sp", None),
        check_vma=False,
    )
```

```python
import functools
import math

import jax
import jax.numpy as jnp
from jax import lax
from jax.experimental import pallas as pl
from jax.experimental.pallas import tpu as pltpu
from jax.sharding import PartitionSpec as P

MESH = pl.DeviceIdType.MESH
F32 = jnp.float32
BF16 = jnp.bfloat16
EPS = 1e-6
ROPE_BASE = 10000.0
GRID_W = 64
RING = 8
XN = 4
TOK = 256
CTXT = 16
D = 2048
HD = 64
NH = 4
QC = NH * HD
LOG2E = 1.4426950408889634


ORDER = [
    (0, 0), (2, 0), (1, 0), (0, -1), (0, 1), (4, 0), (2, -1), (3, 0), (2, 1), (1, 1), (1, -1), (0, -2), (5, 0),
    (6, 0), (4, -1), (4, 1), (3, -1), (2, -2), (3, 1), (0, 2), (7, 0), (1, 2), (1, -2), (0, -3), (6, 1), (5, 1),
    (6, -1), (2, 2), (4, -2), (5, -1), (3, -2), (4, 2), (1, -3), (2, -3), (7, 1), (7, -1), (6, 2), (0, 3),
    (6, -2), (3, 2), (5, 2), (4, -3), (1, 3), (2, 3), (7, -2), (7, 2), (5, -2), (4, 3), (3, 3), (6, -3), (6, 3),
    (5, 3), (7, 3), (7, -3), (0, 4), (1, 4), (4, 4), (2, 4), (3, -3), (3, 4), (6, 4), (5, 4), (7, 4), (5, -3),
]
SLOT = {item: n for n, item in enumerate(ORDER)}
NEXT = {0: ((1, 1), (2, -1)), 1: ((3, 1),), 2: ((4, -1),), 3: ((5, 1),), 4: ((6, -1),), 5: ((7, 1),)}


def onward(item):
    i, r = item
    out = []
    if r == 0:
        out += [(0, way, SLOT[(j, 0)]) for j, way in NEXT.get(i, ())]
    if 0 <= r < 4:
        out.append((1, 1, SLOT[(i, r + 1)]))
    if -3 < r <= 0:
        out.append((1, -1, SLOT[(i, r - 1)]))
    return out


def dot(a, b):
    return jnp.dot(a, b, preferred_element_type=F32)


def kernel(
    latent_h, cond_h, context_h, code_h, shw_h, scw_h, gaw_h, ngain_h, wq_h, wk_h, wv_h, wo_h, qg_h, kg_h, bias_h,
    out_h,
    lat, cond, ctx, code, shw, scw, gaw, ngain, wq, wkv, wo, qg, kg, bias,
    outv, normed, qbd, qctx, buf, mst, alp, acc, att, sbuf0, sbuf1, cbuf0, cbuf1,
    ma, ma_y, ma_s, ma_z, ma_x, mg, mg_y, mg_s, mg_z, mg_x, mb, mb_z, mb_s, mb_y, mb_x,
    lsem, osem, sa, ra, smod, rmod, swo, rwo, satt, ratt,
):
    sp = lax.axis_index("sp")
    x = lax.axis_index("tp")
    d = lax.axis_index("dp")
    z = sp // RING
    y = sp % RING
    sgn = 1 - 2 * d

    def at_y(k):
        return {"sp": z * RING + lax.rem(y + k + 2 * RING, RING)}

    def at_z(k):
        return {"sp": lax.rem(z + k + 2 * RING, RING) * RING + y}

    def at_x(k):
        return {"tp": lax.rem(x + k + 2 * XN, XN)}

    partner = {"dp": 1 - d}

    def remote(src, dst, ss, rs, dev):
        return pltpu.make_async_remote_copy(
            src_ref=src, dst_ref=dst, send_sem=ss, recv_sem=rs, device_id=dev, device_id_type=MESH
        )

    barrier = pltpu.get_barrier_semaphore()
    for k in range(1, RING):
        pl.semaphore_signal(barrier, inc=1, device_id=at_y(k), device_id_type=MESH)
        pl.semaphore_signal(barrier, inc=1, device_id=at_z(k), device_id_type=MESH)
    for k in range(1, XN):
        pl.semaphore_signal(barrier, inc=1, device_id=at_x(k), device_id_type=MESH)
    pl.semaphore_signal(barrier, inc=1, device_id=partner, device_id_type=MESH)

    pairs = [
        (cond_h, cond), (code_h, code), (shw_h, shw), (scw_h, scw), (gaw_h, gaw),
        (latent_h, lat), (context_h, ctx), (ngain_h, ngain), (wk_h, wkv.at[0:HD]), (wv_h, wkv.at[HD : 2 * HD]), (wq_h, wq),
        (qg_h, qg), (kg_h, kg), (bias_h, bias),
        (wo_h.at[:, 0 : D // 2], wo.at[x, 0]), (wo_h.at[:, D // 2 : D], wo.at[x, 1]),
    ]
    loads = [pltpu.make_async_copy(s, t, lsem.at[i]) for i, (s, t) in enumerate(pairs)]
    for c in loads:
        c.start()

    for i in range(5):
        loads[i].wait()
    both = jnp.concatenate([cond[...], code[...]], axis=0).astype(F32)
    act = (both * (1.0 / (1.0 + jnp.exp(-both)))).astype(BF16)
    pshift = dot(act, shw[...])
    pscale = dot(act, scw[...])
    pgate = dot(act, gaw[...])
    for c in range(4):
        cols = slice(c * 128, (c + 1) * 128)
        ma[c : c + 1, :] = pshift[0:1, cols]
        ma[4 + c : 5 + c, :] = pscale[0:1, cols]
        mg[c : c + 1, :] = pgate[0:1, cols]
        mb[c : c + 1, :] = pshift[1:2, cols]
        mb[4 + c : 5 + c, :] = pscale[1:2, cols]
    mg[4:8, :] = jnp.zeros((4, 128), F32)

    pl.semaphore_wait(barrier, 2 * (RING - 1) + (XN - 1) + 1)

    def spread(src, dst, sem, at):
        for k in range(1, RING):
            remote(src, dst.at[k], smod.at[sem], rmod.at[sem], at(k)).start()

    def spread_wait(dst, sem):
        part = dst.at[1:RING]
        remote(part, part, smod.at[sem], rmod.at[sem], at_y(1)).wait()

    spread(ma, ma_y, 0, at_y)
    spread(mb, mb_z, 1, at_z)

    for i in (5, 6, 7, 8, 9):
        loads[i].wait()
    lf = lat[...].astype(F32)
    rms = lax.rsqrt(jnp.mean(lf * lf, axis=-1, keepdims=True) + EPS)
    cf = ctx[...].astype(F32)
    crms = lax.rsqrt(jnp.mean(cf * cf, axis=-1, keepdims=True) + EPS)
    qbd[...] = jnp.zeros(qbd.shape, BF16)
    qctx[...] = jnp.zeros(qctx.shape, BF16)
    mst[...] = jnp.full(mst.shape, -1e30, F32)
    acc[...] = jnp.zeros(acc.shape, F32)
    fi = lax.broadcasted_iota(jnp.int32, (32, TOK), 0)
    ti = lax.broadcasted_iota(jnp.int32, (32, TOK), 1)
    grow = sp * (TOK // GRID_W) + ti // GRID_W
    gcol = ti % GRID_W
    gpos = jnp.where(fi < 16, grow, gcol).astype(F32)
    inv = jnp.exp((fi % 16).astype(F32) * (-math.log(ROPE_BASE) / 16.0))
    angle = gpos * inv
    cosv = jnp.cos(angle)
    sinv = jnp.sin(angle)

    spread_wait(ma_y, 0)
    spread_wait(mb_z, 1)
    ta = ma[...]
    tb = mb[...]
    for k in range(1, RING):
        ta = ta + ma_y[k]
        tb = tb + mb_z[k]
    ma_s[0] = ta
    mb_s[0] = tb
    spread(ma_s.at[0], ma_z, 2, at_z)
    spread(mb_s.at[0], mb_y, 3, at_y)
    spread_wait(ma_z, 2)
    spread_wait(mb_y, 3)
    for k in range(1, RING):
        ta = ta + ma_z[k]
        tb = tb + mb_y[k]
    ma_x[x] = ta
    mb_x[x] = tb
    for k in range(1, XN):
        remote(ma_x.at[x], ma_x.at[x], smod.at[4], rmod.at[4], at_x(k)).start()
        remote(mb_x.at[x], mb_x.at[x], smod.at[5], rmod.at[5], at_x(k)).start()
    for ref, sem in ((ma_x, 4), (mb_x, 5)):
        part = ref.at[1:XN]
        remote(part, part, smod.at[sem], rmod.at[sem], at_x(1)).wait()
    def vec(ref, row):
        return jnp.concatenate([ref[i, row + c : row + c + 1, :] for i in range(XN) for c in range(4)], axis=1)

    gain = ngain[...]
    lshift = vec(ma_x, 0)
    lscale = gain * (1.0 + vec(ma_x, 4))
    cshift = vec(mb_x, 0)
    cscale = gain * (1.0 + vec(mb_x, 4))
    normed[0:TOK, :] = (lat[...].astype(F32) * rms * lscale + lshift).astype(BF16)
    normed[TOK : TOK + CTXT, :] = (cf * crms * cscale + cshift).astype(BF16)

    kv = lax.dot_general(normed[...], wkv[...], (((1,), (1,)), ((), ())), preferred_element_type=F32)
    kvt = kv[0:TOK, :].T
    for i in (10, 11, 12, 13):
        loads[i].wait()
    eye = lax.broadcasted_iota(jnp.int32, (HD, HD), 0) == lax.broadcasted_iota(jnp.int32, (HD, HD), 1)
    qgain = jnp.sum(jnp.where(eye, qg[...], 0.0), axis=1, keepdims=True)
    kgain = jnp.sum(jnp.where(eye, kg[...], 0.0), axis=1, keepdims=True)

    def norm_rope(t, g):
        t = t * lax.rsqrt(jnp.mean(t * t, axis=0, keepdims=True) + EPS) * g
        a, b = t[0:32, :], t[32:64, :]
        return jnp.concatenate([a * cosv - b * sinv, b * cosv + a * sinv], axis=0)

    kt = norm_rope(kvt[0:HD, :], kgain)
    k2 = jnp.concatenate([kt, kt], axis=0).T
    low = lax.broadcasted_iota(jnp.int32, (HD, 128), 1) < HD
    vt = kvt[HD : 2 * HD, :].astype(BF16)
    buf[0, 0:64, :] = jnp.where(low, k2[0:64], k2[64:128]).astype(BF16)
    buf[0, 144:208, :] = jnp.where(low, k2[128:192], k2[192:256]).astype(BF16)
    buf[0, 64:128, :] = vt[:, 0:128]
    buf[0, 208:272, :] = vt[:, 128:256]
    ckv = kv[TOK : TOK + CTXT, :]
    lowc = lax.broadcasted_iota(jnp.int32, (CTXT, 128), 1) < HD
    csq = jnp.sum(jnp.where(lowc, ckv * ckv, 0.0), axis=1, keepdims=True) * (1.0 / HD)
    kg2 = jnp.concatenate([kg[...], kg[...]], axis=1)
    buf[0, 128:144, :] = jnp.where(lowc, ckv * lax.rsqrt(csq + EPS) * kg2, ckv).astype(BF16)

    def ring(axis, k):
        along_y = 1 - d if axis == 0 else d
        k = k * sgn
        return {
            "sp": lax.rem(z + (1 - along_y) * k + RING, RING) * RING + lax.rem(y + along_y * k + RING, RING)
        }

    def group(s):
        return s if s < 16 else 8 + s // 2

    def pass_on(s):
        for axis, way, t in onward(ORDER[s]):
            remote(buf.at[s, 0:144], buf.at[t, 0:144], sa, ra.at[group(t)], ring(axis, way)).start()
            remote(buf.at[s, 144:272], buf.at[t, 144:272], sa, ra.at[group(t)], ring(1 - axis, way)).start()

    def arrived(s, n):
        part = buf.at[s : s + n]
        remote(part, part, sa, ra.at[group(s)], at_z(1)).wait_recv()

    pass_on(0)
    spread(mg, mg_y, 6, at_y)
    for i in (14, 15):
        loads[i].wait()
    wo1 = [
        remote(wo.at[x, d], wo.at[x, d], swo.at[0], rwo.at[0], at_x(1)),
        remote(wo.at[x, d], wo.at[x, d], swo.at[1], rwo.at[1], at_x(-1)),
    ]
    for c in wo1:
        c.start()


    q = dot(normed[0:TOK, :], wq[...])
    qt = q.T
    for h in range(NH):
        qh = norm_rope(qt[h * HD : (h + 1) * HD, :], qgain).astype(BF16)
        qs = qh.astype(F32) * (LOG2E * HD**-0.5)
        hi = qs.astype(BF16)
        lo = (qs - hi.astype(F32)).astype(BF16)
        for t in range(2):
            cols = slice(t * 128, (t + 1) * 128)
            for r, part in ((0, hi), (128, lo)):
                qbd[2 * h + t, r : r + 64, 0:128] = part[:, cols]
                qbd[2 * h + t, r + 64 : r + 128, 128:256] = part[:, cols]
        qctx[h, 0:64, :] = hi
        qctx[h, 128:192, :] = lo

    sbuf = (sbuf0, sbuf1)
    cbuf = (cbuf0, cbuf1)

    def keep(keys, ctxs, h, n):
        sc = dot(ctxs, qctx[h]) + bias[0:1, h : h + 1] * LOG2E
        cbuf[n][0] = sc
        mc = jnp.max(sc.reshape(8, 8, 256), axis=0)
        for t in range(2):
            sc = dot(keys, qbd[2 * h + t])
            sbuf[n][:, :, t * 256 : (t + 1) * 256] = sc.reshape(4, 128, 256)
            m = jnp.max(sc.reshape(64, 8, 256), axis=0)
            cols = slice(t * 128, (t + 1) * 128)
            m = jnp.maximum(jnp.maximum(m[:, 0:128], m[:, 128:256]), mc[:, cols])
            mold = mst[h, :, cols]
            m = jnp.maximum(jnp.broadcast_to(jnp.max(m, axis=0, keepdims=True), (8, 128)), mold)
            mst[h, :, cols] = m
            alp[h, :, cols] = jnp.exp2(mold - m)

    def use(vals, cvals, h, n, zero):
        m = mst[h]
        e = jnp.exp2(cbuf[n][zero].reshape(8, 8, 256) - m[None])
        prod = dot(cvals, e.reshape(64, 256).astype(BF16))
        m = jnp.concatenate([m[:, 0:128]] * 2 + [m[:, 128:256]] * 2, axis=1)
        for k in range(4):
            e = jnp.exp2(sbuf[n][k + zero].reshape(16, 8, 512) - m[None])
            pb = e.reshape(128, 512).astype(BF16)
            p = jnp.concatenate(
                [
                    jnp.concatenate([pb[r : r + 64, c : c + 128], pb[r : r + 64, c + 256 : c + 384]], axis=1)
                    for r in (0, 64)
                    for c in (0, 128)
                ],
                axis=0,
            )
            prod = prod + dot(vals[:, 256 * k : 256 * k + 256], p)
        acc[h] = acc[h] * alp[h, 0:1, :] + prod

    def receive(st):
        n = 1 if st < 4 else 2
        for s in range(4 * st, 4 * st + 4, n):
            if s > 0:
                arrived(s, n)
                for t in range(n):
                    pass_on(s + t)

    def pick(value, low, high):
        if high - low == 1:
            receive(low)
            return
        mid = (low + high) // 2

        @pl.when(value < mid)
        def _():
            pick(value, low, mid)

        @pl.when(value >= mid)
        def _():
            pick(value, mid, high)

    def keys_of(base):
        k = jnp.concatenate(
            [buf[pl.ds(base, 4), 0:64, :].reshape(256, 128), buf[pl.ds(base, 4), 144:208, :].reshape(256, 128)], axis=0
        )
        return jnp.concatenate([k, k], axis=1)

    def step(it, carry):
        base = it * 4
        zero = jnp.minimum(it, 0)

        pick(it, 0, 16)

        @pl.when(it == 5)
        def _():
            spread_wait(mg_y, 6)
            tg = mg[...]
            for k in range(1, RING):
                tg = tg + mg_y[k]
            mg_s[0] = tg
            spread(mg_s.at[0], mg_z, 7, at_z)

        @pl.when(it == 12)
        def _():
            spread_wait(mg_z, 7)
            tg = mg_s[0]
            for k in range(1, RING):
                tg = tg + mg_z[k]
            mg_x[x] = tg
            for k in range(1, XN):
                remote(mg_x.at[x], mg_x.at[x], smod.at[8], rmod.at[8], at_x(k)).start()

        @pl.when(it == 8)
        def _():
            for c in wo1:
                c.wait()
            left = lax.rem(x + XN - 1, XN)
            right = lax.rem(x + 1, XN)
            remote(wo.at[left, d, 0:128], wo.at[left, d, 0:128], swo.at[2], rwo.at[2], at_x(1)).start()
            remote(wo.at[right, d, 128:256], wo.at[right, d, 128:256], swo.at[3], rwo.at[3], at_x(-1)).start()
            remote(wo.at[left, d], wo.at[left, d], swo.at[4], rwo.at[4], partner).start()
            remote(wo.at[right, d], wo.at[right, d], swo.at[5], rwo.at[5], partner).start()

        @pl.when(it == 14)
        def _():
            far = lax.rem(x + 2, XN)
            remote(wo.at[far, d, 0:128], wo.at[far, d, 0:128], swo.at[2], rwo.at[2], at_x(1)).wait()
            remote(wo.at[far, d, 128:256], wo.at[far, d, 128:256], swo.at[3], rwo.at[3], at_x(-1)).wait()
            remote(wo.at[far, d], wo.at[far, d], swo.at[6], rwo.at[6], partner).start()

        keys = keys_of(base)
        vals = jnp.concatenate(
            [buf[base + k, 64:128, :] for k in range(4)] + [buf[base + k, 208:272, :] for k in range(4)], axis=1
        )
        vals = jnp.concatenate([vals, jnp.ones((16, 1024), BF16)], axis=0)
        ctxs = buf[pl.ds(base, 4), 128:144, :].reshape(64, 128)
        cvals = jnp.concatenate([ctxs.astype(F32).T[HD:128, :].astype(BF16), jnp.ones((16, 64), BF16)], axis=0)
        ctxs = jnp.concatenate([ctxs, ctxs], axis=1)
        keep(keys, ctxs, 0, 0)
        for h in range(NH):
            if h + 1 < NH:
                keep(keys, ctxs, h + 1, (h + 1) % 2)
            use(vals, cvals, h, h % 2, zero)

        return carry

    lax.fori_loop(0, 16, step, 0)

    heads = []
    for h in range(NH):
        heads.append(acc[h, 0:HD] / acc[h, HD : HD + 1])
    att[x] = jnp.concatenate(heads, axis=0).T.astype(BF16)

    left = lax.rem(x + XN - 1, XN)
    right = lax.rem(x + 1, XN)
    far = lax.rem(x + 2, XN)

    def att_copy(slot, half, sem, k):
        part = att.at[slot, half * 128 : half * 128 + 128]
        return remote(part, part, satt.at[sem], ratt.at[sem], at_x(k))

    own = [att_copy(x, 0, 0, 1), att_copy(x, 1, 1, -1), att_copy(x, 1, 2, 1), att_copy(x, 0, 3, -1)]
    for c in own:
        c.start()
    part = buf.at[1:64]
    remote(part, part, sa, ra.at[0], at_z(1)).wait_send()
    own[0].wait_recv()
    fwd0 = att_copy(left, 0, 4, 1)
    fwd0.start()
    own[1].wait_recv()
    fwd1 = att_copy(right, 1, 5, -1)
    fwd1.start()
    own[2].wait_recv()
    own[3].wait_recv()
    for s, slot in ((4, left), (5, right), (6, far)):
        remote(wo.at[slot, d], wo.at[slot, d], swo.at[s], rwo.at[s], partner).wait()
    fwd0.wait()
    fwd1.wait()

    piece = mg_x.at[1:XN]
    remote(piece, piece, smod.at[8], rmod.at[8], at_x(1)).wait()
    gate = vec(mg_x, 0)
    for c in range(8):
        side, off = c // 4, (c % 4) * 256
        mixed = jnp.zeros((TOK, 256), F32)
        for g in range(XN):
            mixed = mixed + dot(att[g], wo[g, side, :, off : off + 256]).astype(BF16).astype(F32)
        cols = slice(c * 256, (c + 1) * 256)
        outv[:, cols] = (lat[:, cols].astype(F32) + gate[:, cols] * mixed).astype(BF16)
        pltpu.make_async_copy(outv.at[:, cols], out_h.at[:, cols], osem).start()

    for c in own:
        c.wait_send()

    pltpu.make_async_copy(outv, out_h, osem).wait()


def on_device(
    latent, condition, context, context_code, shift_weight, scale_weight, gate_weight, norm_gain,
    query_weight, key_weight, value_weight, output_weight, query_gain, key_gain, context_bias,
):
    V = pltpu.VMEM
    dma = pltpu.SemaphoreType.DMA
    scratch = [
        V((TOK, D), BF16), V((1, 32), BF16), V((CTXT, D), BF16), V((1, 32), BF16),
        V((32, 512), BF16), V((32, 512), BF16), V((32, 512), BF16), V((1, D), F32),
        V((D, QC), BF16), V((2 * HD, D), BF16), V((XN, 2, QC, D // 2), BF16),
        V((1, HD), F32), V((1, HD), F32), V((1, NH), F32),
        V((TOK, D), BF16), V((TOK + CTXT, D), BF16),
        V((8, 256, 256), BF16), V((NH, 256, 256), BF16),
        V((64, 272, 128), BF16),
        V((NH, 8, 256), F32), V((NH, 8, 256), F32), V((NH, HD + 16, 256), F32), V((XN, TOK, QC), BF16),
        V((4, 128, 512), F32), V((4, 128, 512), F32), V((1, 64, 256), F32), V((1, 64, 256), F32),
        V((8, 128), F32), V((RING, 8, 128), F32), V((1, 8, 128), F32), V((RING, 8, 128), F32), V((XN, 8, 128), F32),
        V((8, 128), F32), V((RING, 8, 128), F32), V((1, 8, 128), F32), V((RING, 8, 128), F32), V((XN, 8, 128), F32),
        V((8, 128), F32), V((RING, 8, 128), F32), V((1, 8, 128), F32), V((RING, 8, 128), F32), V((XN, 8, 128), F32),
        dma((16,)), dma, dma, dma((40,)),
        dma((9,)), dma((9,)), dma((7,)), dma((7,)), dma((6,)), dma((6,)),
    ]
    out = pl.pallas_call(
        kernel,
        out_shape=jax.ShapeDtypeStruct((TOK, D), BF16),
        in_specs=[pl.BlockSpec(memory_space=pl.ANY)] * 15,
        out_specs=pl.BlockSpec(memory_space=pl.ANY),
        scratch_shapes=scratch,
        compiler_params=pltpu.CompilerParams(
            collective_id=0, has_side_effects=True, vmem_limit_bytes=60 * 1024 * 1024
        ),
        name="fused",
    )(
        latent[0], condition, context[0], context_code[None], shift_weight, scale_weight, gate_weight,
        norm_gain[None], query_weight, key_weight.T, value_weight.T, output_weight,
        query_gain[None], key_gain[None], context_bias[None],
    )
    return out[None]


def solution(mesh):
    return jax.shard_map(
        on_device,
        mesh=mesh,
        in_specs=(
            P("dp", "sp", None), P("dp", "sp"), P("dp", "sp", None), P("sp"),
            P("sp", "tp"), P("sp", "tp"), P("sp", "tp"), P(),
            P(None, "tp"), P(None, "tp"), P(None, "tp"), P("tp", None),
            P(), P(), P("tp"),
        ),
        out_specs=P("dp", "sp", None),
        check_vma=False,
    )
```

```python
import functools
import math

import jax
import jax.numpy as jnp
from jax import lax
from jax.experimental import pallas as pl
from jax.experimental.pallas import tpu as pltpu
from jax.sharding import PartitionSpec as P

MESH = pl.DeviceIdType.MESH
F32 = jnp.float32
BF16 = jnp.bfloat16
EPS = 1e-6
ROPE_BASE = 10000.0
GRID_W = 64
RING = 8
XN = 4
TOK = 256
CTXT = 16
D = 2048
HD = 64
NH = 4
QC = NH * HD
LOG2E = 1.4426950408889634


ORDER = [
    (0, 0), (2, 0), (1, 0), (0, -1), (0, 1), (4, 0), (2, -1), (3, 0), (2, 1), (1, 1), (1, -1), (0, -2), (5, 0),
    (6, 0), (4, -1), (4, 1), (3, -1), (2, -2), (3, 1), (0, 2), (7, 0), (1, 2), (1, -2), (0, -3), (6, 1), (5, 1),
    (6, -1), (2, 2), (4, -2), (5, -1), (3, -2), (4, 2), (1, -3), (2, -3), (7, 1), (7, -1), (6, 2), (0, 3),
    (6, -2), (3, 2), (5, 2), (4, -3), (1, 3), (2, 3), (7, -2), (7, 2), (5, -2), (4, 3), (3, 3), (6, -3), (6, 3),
    (5, 3), (7, 3), (7, -3), (0, 4), (1, 4), (4, 4), (2, 4), (3, -3), (3, 4), (6, 4), (5, 4), (7, 4), (5, -3),
]
SLOT = {item: n for n, item in enumerate(ORDER)}
NEXT = {0: ((1, 1), (2, -1)), 1: ((3, 1),), 2: ((4, -1),), 3: ((5, 1),), 4: ((6, -1),), 5: ((7, 1),)}


def onward(item):
    i, r = item
    out = []
    if r == 0:
        out += [(0, way, SLOT[(j, 0)]) for j, way in NEXT.get(i, ())]
    if 0 <= r < 4:
        out.append((1, 1, SLOT[(i, r + 1)]))
    if -3 < r <= 0:
        out.append((1, -1, SLOT[(i, r - 1)]))
    return out


def dot(a, b):
    return jnp.dot(a, b, preferred_element_type=F32)


def kernel(
    latent_h, cond_h, context_h, code_h, shw_h, scw_h, gaw_h, ngain_h, wq_h, wk_h, wv_h, wo_h, qg_h, kg_h, bias_h,
    out_h,
    lat, cond, ctx, code, shw, scw, gaw, ngain, wq, wkv, wo, qg, kg, bias,
    outv, normed, qbd, qctx, buf, mst, alp, acc, att, sbuf0, sbuf1, sbuf2, cbuf0, cbuf1, cbuf2,
    ma, ma_y, ma_s, ma_z, ma_x, mg, mg_y, mg_s, mg_z, mg_x, mb, mb_z, mb_s, mb_y, mb_x,
    lsem, osem, sa, ra, smod, rmod, swo, rwo, satt, ratt,
):
    sp = lax.axis_index("sp")
    x = lax.axis_index("tp")
    d = lax.axis_index("dp")
    z = sp // RING
    y = sp % RING
    sgn = 1 - 2 * d

    def at_y(k):
        return {"sp": z * RING + lax.rem(y + k + 2 * RING, RING)}

    def at_z(k):
        return {"sp": lax.rem(z + k + 2 * RING, RING) * RING + y}

    def at_x(k):
        return {"tp": lax.rem(x + k + 2 * XN, XN)}

    partner = {"dp": 1 - d}

    def remote(src, dst, ss, rs, dev):
        return pltpu.make_async_remote_copy(
            src_ref=src, dst_ref=dst, send_sem=ss, recv_sem=rs, device_id=dev, device_id_type=MESH
        )

    barrier = pltpu.get_barrier_semaphore()
    for k in range(1, RING):
        pl.semaphore_signal(barrier, inc=1, device_id=at_y(k), device_id_type=MESH)
        pl.semaphore_signal(barrier, inc=1, device_id=at_z(k), device_id_type=MESH)
    for k in range(1, XN):
        pl.semaphore_signal(barrier, inc=1, device_id=at_x(k), device_id_type=MESH)
    pl.semaphore_signal(barrier, inc=1, device_id=partner, device_id_type=MESH)

    pairs = [
        (cond_h, cond), (code_h, code), (shw_h, shw), (scw_h, scw), (gaw_h, gaw),
        (latent_h, lat), (context_h, ctx), (ngain_h, ngain), (wk_h, wkv.at[0:HD]), (wv_h, wkv.at[HD : 2 * HD]), (wq_h, wq),
        (qg_h, qg), (kg_h, kg), (bias_h, bias),
        (wo_h.at[:, 0 : D // 2], wo.at[x, 0]), (wo_h.at[:, D // 2 : D], wo.at[x, 1]),
    ]
    loads = [pltpu.make_async_copy(s, t, lsem.at[i]) for i, (s, t) in enumerate(pairs)]
    for c in loads:
        c.start()

    for i in range(5):
        loads[i].wait()
    both = jnp.concatenate([cond[...], code[...]], axis=0).astype(F32)
    act = (both * (1.0 / (1.0 + jnp.exp(-both)))).astype(BF16)
    pshift = dot(act, shw[...])
    pscale = dot(act, scw[...])
    pgate = dot(act, gaw[...])
    for c in range(4):
        cols = slice(c * 128, (c + 1) * 128)
        ma[c : c + 1, :] = pshift[0:1, cols]
        ma[4 + c : 5 + c, :] = pscale[0:1, cols]
        mg[c : c + 1, :] = pgate[0:1, cols]
        mb[c : c + 1, :] = pshift[1:2, cols]
        mb[4 + c : 5 + c, :] = pscale[1:2, cols]
    mg[4:8, :] = jnp.zeros((4, 128), F32)

    pl.semaphore_wait(barrier, 2 * (RING - 1) + (XN - 1) + 1)

    def spread(src, dst, sem, at):
        for k in range(1, RING):
            remote(src, dst.at[k], smod.at[sem], rmod.at[sem], at(k)).start()

    def spread_wait(dst, sem):
        part = dst.at[1:RING]
        remote(part, part, smod.at[sem], rmod.at[sem], at_y(1)).wait()

    spread(ma, ma_y, 0, at_y)
    spread(mb, mb_z, 1, at_z)

    for i in (5, 6, 7, 8, 9):
        loads[i].wait()
    lf = lat[...].astype(F32)
    rms = lax.rsqrt(jnp.mean(lf * lf, axis=-1, keepdims=True) + EPS)
    cf = ctx[...].astype(F32)
    crms = lax.rsqrt(jnp.mean(cf * cf, axis=-1, keepdims=True) + EPS)
    qbd[...] = jnp.zeros(qbd.shape, BF16)
    qctx[...] = jnp.zeros(qctx.shape, BF16)
    mst[...] = jnp.full(mst.shape, -1e30, F32)
    acc[...] = jnp.zeros(acc.shape, F32)
    fi = lax.broadcasted_iota(jnp.int32, (32, TOK), 0)
    ti = lax.broadcasted_iota(jnp.int32, (32, TOK), 1)
    grow = sp * (TOK // GRID_W) + ti // GRID_W
    gcol = ti % GRID_W
    gpos = jnp.where(fi < 16, grow, gcol).astype(F32)
    inv = jnp.exp((fi % 16).astype(F32) * (-math.log(ROPE_BASE) / 16.0))
    angle = gpos * inv
    cosv = jnp.cos(angle)
    sinv = jnp.sin(angle)

    spread_wait(ma_y, 0)
    spread_wait(mb_z, 1)
    ta = ma[...]
    tb = mb[...]
    for k in range(1, RING):
        ta = ta + ma_y[k]
        tb = tb + mb_z[k]
    ma_s[0] = ta
    mb_s[0] = tb
    spread(ma_s.at[0], ma_z, 2, at_z)
    spread(mb_s.at[0], mb_y, 3, at_y)
    spread_wait(ma_z, 2)
    spread_wait(mb_y, 3)
    for k in range(1, RING):
        ta = ta + ma_z[k]
        tb = tb + mb_y[k]
    ma_x[x] = ta
    mb_x[x] = tb
    for k in range(1, XN):
        remote(ma_x.at[x], ma_x.at[x], smod.at[4], rmod.at[4], at_x(k)).start()
        remote(mb_x.at[x], mb_x.at[x], smod.at[5], rmod.at[5], at_x(k)).start()
    for ref, sem in ((ma_x, 4), (mb_x, 5)):
        part = ref.at[1:XN]
        remote(part, part, smod.at[sem], rmod.at[sem], at_x(1)).wait()
    def vec(ref, row):
        return jnp.concatenate([ref[i, row + c : row + c + 1, :] for i in range(XN) for c in range(4)], axis=1)

    gain = ngain[...]
    lshift = vec(ma_x, 0)
    lscale = gain * (1.0 + vec(ma_x, 4))
    cshift = vec(mb_x, 0)
    cscale = gain * (1.0 + vec(mb_x, 4))
    normed[0:TOK, :] = (lat[...].astype(F32) * rms * lscale + lshift).astype(BF16)
    normed[TOK : TOK + CTXT, :] = (cf * crms * cscale + cshift).astype(BF16)

    kv = lax.dot_general(normed[...], wkv[...], (((1,), (1,)), ((), ())), preferred_element_type=F32)
    kvt = kv[0:TOK, :].T
    for i in (10, 11, 12, 13):
        loads[i].wait()
    eye = lax.broadcasted_iota(jnp.int32, (HD, HD), 0) == lax.broadcasted_iota(jnp.int32, (HD, HD), 1)
    qgain = jnp.sum(jnp.where(eye, qg[...], 0.0), axis=1, keepdims=True)
    kgain = jnp.sum(jnp.where(eye, kg[...], 0.0), axis=1, keepdims=True)

    def norm_rope(t, g):
        t = t * lax.rsqrt(jnp.mean(t * t, axis=0, keepdims=True) + EPS) * g
        a, b = t[0:32, :], t[32:64, :]
        return jnp.concatenate([a * cosv - b * sinv, b * cosv + a * sinv], axis=0)

    kt = norm_rope(kvt[0:HD, :], kgain)
    k2 = jnp.concatenate([kt, kt], axis=0).T
    low = lax.broadcasted_iota(jnp.int32, (HD, 128), 1) < HD
    vt = kvt[HD : 2 * HD, :].astype(BF16)
    buf[0, 0:64, :] = jnp.where(low, k2[0:64], k2[64:128]).astype(BF16)
    buf[0, 144:208, :] = jnp.where(low, k2[128:192], k2[192:256]).astype(BF16)
    buf[0, 64:128, :] = vt[:, 0:128]
    buf[0, 208:272, :] = vt[:, 128:256]
    ckv = kv[TOK : TOK + CTXT, :]
    lowc = lax.broadcasted_iota(jnp.int32, (CTXT, 128), 1) < HD
    csq = jnp.sum(jnp.where(lowc, ckv * ckv, 0.0), axis=1, keepdims=True) * (1.0 / HD)
    kg2 = jnp.concatenate([kg[...], kg[...]], axis=1)
    buf[0, 128:144, :] = jnp.where(lowc, ckv * lax.rsqrt(csq + EPS) * kg2, ckv).astype(BF16)

    def ring(axis, k):
        along_y = 1 - d if axis == 0 else d
        k = k * sgn
        return {
            "sp": lax.rem(z + (1 - along_y) * k + RING, RING) * RING + lax.rem(y + along_y * k + RING, RING)
        }

    def group(s):
        return s if s < 16 else 8 + s // 2

    def pass_on(s):
        for axis, way, t in onward(ORDER[s]):
            remote(buf.at[s, 0:144], buf.at[t, 0:144], sa, ra.at[group(t)], ring(axis, way)).start()
            remote(buf.at[s, 144:272], buf.at[t, 144:272], sa, ra.at[group(t)], ring(1 - axis, way)).start()

    def arrived(s, n):
        part = buf.at[s : s + n]
        remote(part, part, sa, ra.at[group(s)], at_z(1)).wait_recv()

    pass_on(0)
    spread(mg, mg_y, 6, at_y)
    for i in (14, 15):
        loads[i].wait()
    wo1 = [
        remote(wo.at[x, d], wo.at[x, d], swo.at[0], rwo.at[0], at_x(1)),
        remote(wo.at[x, d], wo.at[x, d], swo.at[1], rwo.at[1], at_x(-1)),
    ]
    for c in wo1:
        c.start()


    q = dot(normed[0:TOK, :], wq[...])
    qt = q.T
    for h in range(NH):
        qh = norm_rope(qt[h * HD : (h + 1) * HD, :], qgain).astype(BF16)
        qs = qh.astype(F32) * (LOG2E * HD**-0.5)
        hi = qs.astype(BF16)
        lo = (qs - hi.astype(F32)).astype(BF16)
        for t in range(2):
            cols = slice(t * 128, (t + 1) * 128)
            for r, part in ((0, hi), (128, lo)):
                qbd[2 * h + t, r : r + 64, 0:128] = part[:, cols]
                qbd[2 * h + t, r + 64 : r + 128, 128:256] = part[:, cols]
        qctx[h, 0:64, :] = hi
        qctx[h, 128:192, :] = lo

    sbuf = (sbuf0, sbuf1, sbuf2)
    cbuf = (cbuf0, cbuf1, cbuf2)

    def keep(keys, ctxs, h, n):
        sc = dot(ctxs, qctx[h]) + bias[0:1, h : h + 1] * LOG2E
        cbuf[n][0] = sc
        mc = jnp.max(sc.reshape(8, 8, 256), axis=0)
        for t in range(2):
            sc = dot(keys, qbd[2 * h + t])
            sbuf[n][:, :, t * 256 : (t + 1) * 256] = sc.reshape(4, 128, 256)
            m = jnp.max(sc.reshape(64, 8, 256), axis=0)
            cols = slice(t * 128, (t + 1) * 128)
            m = jnp.maximum(jnp.maximum(m[:, 0:128], m[:, 128:256]), mc[:, cols])
            mold = mst[h, :, cols]
            m = jnp.maximum(jnp.broadcast_to(jnp.max(m, axis=0, keepdims=True), (8, 128)), mold)
            mst[h, :, cols] = m
            alp[h, :, cols] = jnp.exp2(mold - m)

    def use(vals, cvals, h, n, zero):
        m = mst[h]
        e = jnp.exp2(cbuf[n][zero].reshape(8, 8, 256) - m[None])
        prod = dot(cvals, e.reshape(64, 256).astype(BF16))
        m = jnp.concatenate([m[:, 0:128]] * 2 + [m[:, 128:256]] * 2, axis=1)
        for k in range(4):
            e = jnp.exp2(sbuf[n][k + zero].reshape(16, 8, 512) - m[None])
            pb = e.reshape(128, 512).astype(BF16)
            p = jnp.concatenate(
                [
                    jnp.concatenate([pb[r : r + 64, c : c + 128], pb[r : r + 64, c + 256 : c + 384]], axis=1)
                    for r in (0, 64)
                    for c in (0, 128)
                ],
                axis=0,
            )
            prod = prod + dot(vals[:, 256 * k : 256 * k + 256], p)
        acc[h] = acc[h] * alp[h, 0:1, :] + prod

    def receive(st):
        n = 1 if st < 4 else 2
        for s in range(4 * st, 4 * st + 4, n):
            if s > 0:
                arrived(s, n)
                for t in range(n):
                    pass_on(s + t)

    def pick(value, low, high):
        if high - low == 1:
            receive(low)
            return
        mid = (low + high) // 2

        @pl.when(value < mid)
        def _():
            pick(value, low, mid)

        @pl.when(value >= mid)
        def _():
            pick(value, mid, high)

    def keys_of(base):
        k = jnp.concatenate(
            [buf[pl.ds(base, 4), 0:64, :].reshape(256, 128), buf[pl.ds(base, 4), 144:208, :].reshape(256, 128)], axis=0
        )
        return jnp.concatenate([k, k], axis=1)

    def step(it, carry):
        base = it * 4
        zero = jnp.minimum(it, 0)

        pick(it, 0, 16)

        @pl.when(it == 5)
        def _():
            spread_wait(mg_y, 6)
            tg = mg[...]
            for k in range(1, RING):
                tg = tg + mg_y[k]
            mg_s[0] = tg
            spread(mg_s.at[0], mg_z, 7, at_z)

        @pl.when(it == 12)
        def _():
            spread_wait(mg_z, 7)
            tg = mg_s[0]
            for k in range(1, RING):
                tg = tg + mg_z[k]
            mg_x[x] = tg
            for k in range(1, XN):
                remote(mg_x.at[x], mg_x.at[x], smod.at[8], rmod.at[8], at_x(k)).start()

        @pl.when(it == 8)
        def _():
            for c in wo1:
                c.wait()
            left = lax.rem(x + XN - 1, XN)
            right = lax.rem(x + 1, XN)
            remote(wo.at[left, d, 0:128], wo.at[left, d, 0:128], swo.at[2], rwo.at[2], at_x(1)).start()
            remote(wo.at[right, d, 128:256], wo.at[right, d, 128:256], swo.at[3], rwo.at[3], at_x(-1)).start()
            remote(wo.at[left, d], wo.at[left, d], swo.at[4], rwo.at[4], partner).start()
            remote(wo.at[right, d], wo.at[right, d], swo.at[5], rwo.at[5], partner).start()

        @pl.when(it == 14)
        def _():
            far = lax.rem(x + 2, XN)
            remote(wo.at[far, d, 0:128], wo.at[far, d, 0:128], swo.at[2], rwo.at[2], at_x(1)).wait()
            remote(wo.at[far, d, 128:256], wo.at[far, d, 128:256], swo.at[3], rwo.at[3], at_x(-1)).wait()
            remote(wo.at[far, d], wo.at[far, d], swo.at[6], rwo.at[6], partner).start()

        keys = keys_of(base)
        vals = jnp.concatenate(
            [buf[base + k, 64:128, :] for k in range(4)] + [buf[base + k, 208:272, :] for k in range(4)], axis=1
        )
        vals = jnp.concatenate([vals, jnp.ones((16, 1024), BF16)], axis=0)
        ctxs = buf[pl.ds(base, 4), 128:144, :].reshape(64, 128)
        cvals = jnp.concatenate([ctxs.astype(F32).T[HD:128, :].astype(BF16), jnp.ones((16, 64), BF16)], axis=0)
        ctxs = jnp.concatenate([ctxs, ctxs], axis=1)
        keep(keys, ctxs, 0, 0)
        keep(keys, ctxs, 1, 1)
        for h in range(NH):
            if h + 2 < NH:
                keep(keys, ctxs, h + 2, (h + 2) % 3)
            use(vals, cvals, h, h % 3, zero)

        return carry

    lax.fori_loop(0, 16, step, 0)

    heads = []
    for h in range(NH):
        heads.append(acc[h, 0:HD] / acc[h, HD : HD + 1])
    att[x] = jnp.concatenate(heads, axis=0).T.astype(BF16)

    left = lax.rem(x + XN - 1, XN)
    right = lax.rem(x + 1, XN)
    far = lax.rem(x + 2, XN)

    def att_copy(slot, half, sem, k):
        part = att.at[slot, half * 128 : half * 128 + 128]
        return remote(part, part, satt.at[sem], ratt.at[sem], at_x(k))

    own = [att_copy(x, 0, 0, 1), att_copy(x, 1, 1, -1), att_copy(x, 1, 2, 1), att_copy(x, 0, 3, -1)]
    for c in own:
        c.start()
    part = buf.at[1:64]
    remote(part, part, sa, ra.at[0], at_z(1)).wait_send()
    own[0].wait_recv()
    fwd0 = att_copy(left, 0, 4, 1)
    fwd0.start()
    own[1].wait_recv()
    fwd1 = att_copy(right, 1, 5, -1)
    fwd1.start()
    own[2].wait_recv()
    own[3].wait_recv()
    for s, slot in ((4, left), (5, right), (6, far)):
        remote(wo.at[slot, d], wo.at[slot, d], swo.at[s], rwo.at[s], partner).wait()
    fwd0.wait()
    fwd1.wait()

    piece = mg_x.at[1:XN]
    remote(piece, piece, smod.at[8], rmod.at[8], at_x(1)).wait()
    gate = vec(mg_x, 0)
    for c in range(8):
        side, off = c // 4, (c % 4) * 256
        mixed = jnp.zeros((TOK, 256), F32)
        for g in range(XN):
            mixed = mixed + dot(att[g], wo[g, side, :, off : off + 256]).astype(BF16).astype(F32)
        cols = slice(c * 256, (c + 1) * 256)
        outv[:, cols] = (lat[:, cols].astype(F32) + gate[:, cols] * mixed).astype(BF16)
        pltpu.make_async_copy(outv.at[:, cols], out_h.at[:, cols], osem).start()

    for c in own:
        c.wait_send()

    pltpu.make_async_copy(outv, out_h, osem).wait()


def on_device(
    latent, condition, context, context_code, shift_weight, scale_weight, gate_weight, norm_gain,
    query_weight, key_weight, value_weight, output_weight, query_gain, key_gain, context_bias,
):
    V = pltpu.VMEM
    dma = pltpu.SemaphoreType.DMA
    scratch = [
        V((TOK, D), BF16), V((1, 32), BF16), V((CTXT, D), BF16), V((1, 32), BF16),
        V((32, 512), BF16), V((32, 512), BF16), V((32, 512), BF16), V((1, D), F32),
        V((D, QC), BF16), V((2 * HD, D), BF16), V((XN, 2, QC, D // 2), BF16),
        V((1, HD), F32), V((1, HD), F32), V((1, NH), F32),
        V((TOK, D), BF16), V((TOK + CTXT, D), BF16),
        V((8, 256, 256), BF16), V((NH, 256, 256), BF16),
        V((64, 272, 128), BF16),
        V((NH, 8, 256), F32), V((NH, 8, 256), F32), V((NH, HD + 16, 256), F32), V((XN, TOK, QC), BF16),
        V((4, 128, 512), F32), V((4, 128, 512), F32), V((4, 128, 512), F32), V((1, 64, 256), F32), V((1, 64, 256), F32), V((1, 64, 256), F32),
        V((8, 128), F32), V((RING, 8, 128), F32), V((1, 8, 128), F32), V((RING, 8, 128), F32), V((XN, 8, 128), F32),
        V((8, 128), F32), V((RING, 8, 128), F32), V((1, 8, 128), F32), V((RING, 8, 128), F32), V((XN, 8, 128), F32),
        V((8, 128), F32), V((RING, 8, 128), F32), V((1, 8, 128), F32), V((RING, 8, 128), F32), V((XN, 8, 128), F32),
        dma((16,)), dma, dma, dma((40,)),
        dma((9,)), dma((9,)), dma((7,)), dma((7,)), dma((6,)), dma((6,)),
    ]
    out = pl.pallas_call(
        kernel,
        out_shape=jax.ShapeDtypeStruct((TOK, D), BF16),
        in_specs=[pl.BlockSpec(memory_space=pl.ANY)] * 15,
        out_specs=pl.BlockSpec(memory_space=pl.ANY),
        scratch_shapes=scratch,
        compiler_params=pltpu.CompilerParams(
            collective_id=0, has_side_effects=True, vmem_limit_bytes=60 * 1024 * 1024
        ),
        name="fused",
    )(
        latent[0], condition, context[0], context_code[None], shift_weight, scale_weight, gate_weight,
        norm_gain[None], query_weight, key_weight.T, value_weight.T, output_weight,
        query_gain[None], key_gain[None], context_bias[None],
    )
    return out[None]


def solution(mesh):
    return jax.shard_map(
        on_device,
        mesh=mesh,
        in_specs=(
            P("dp", "sp", None), P("dp", "sp"), P("dp", "sp", None), P("sp"),
            P("sp", "tp"), P("sp", "tp"), P("sp", "tp"), P(),
            P(None, "tp"), P(None, "tp"), P(None, "tp"), P("tp", None),
            P(), P(), P("tp"),
        ),
        out_specs=P("dp", "sp", None),
        check_vma=False,
    )
```
